512 devices in a mesh: grp: 2 (over y), fs: 32 (over z), tp: 8 (over x, core).
Axes of the slice: x: 4, y: 2, z: 32, core: 2. Of those that a mesh axis runs over, the one named last changes fastest.
The devices are a block of a 4x8x32 slice.
Arguments:
- tokens: bfloat16 [32768, 2048], P(('grp', 'fs')), parts along dimension 0, may hold values from -6 to 6
- pre_gain: float32 [2048], replicated, may hold values from 0.1 to 1.9
- up_weight: float32 [2048, 8192], P('fs', 'tp'), may hold values from -0.125 to 0.125
- up_scale: float32 [8192], P('tp'), may hold values from 0.3 to 3
- down_weight: float32 [8192, 2048], P('tp', 'fs'), may hold values from -0.0625 to 0.0625
- down_scale: float32 [2048], P('fs'), may hold values from 0.3 to 3
- post_gain: float32 [2048], replicated, may hold values from 0.1 to 1.9
Outputs:
- mixed: bfloat16 [32768, 2048], P(('grp', 'fs')), parts along dimension 0
The draws below stay inside these ranges and needn't reach their ends.
There are 2 independent parts, one for each index of `grp`. The reference program is written for one: setup_inputs(seed, part) draws one part's arguments, and reference() takes and returns one part's arrays. A program takes and returns all parts, laid end to end along the dimension named above; an argument that names none is the same for every part. Nothing has to cross between parts.
All inputs are finite; a program needn't handle non-finite values.
Results may differ from the reference program's by a relative error of at most 0.01.
Values may be sent and summed in bfloat16 or wider, within the bound.
A program may use at most 64 MiB of HBM per device.

```python
import math
import jax
import jax.numpy as jnp
from jax import lax

D = 2048
FF = 8192
TOK_DEV = 512
TOKENS = 16384
N_FS = 32
N_TP = 8


def levels(rng, shape, cuts, least, top_value):
    def one(dim, blocks):
        steps = jax.random.uniform(jax.random.fold_in(jax.random.fold_in(rng, 6), dim), (blocks,), jnp.float32, least / len(cuts), top_value / len(cuts))
        return jnp.repeat(jnp.exp(steps), shape[dim] // blocks).reshape((-1,) + (1,) * (len(shape) - dim - 1))

    gain = one(*cuts[0])
    for cut in cuts[1:]:
        gain = gain * one(*cut)
    return gain


def scatter_about(key, shape, scale, limit, split=(), dtype=jnp.bfloat16):
    gain = levels(key, shape, split, -0.22, 0.18) if split else 1.0
    values = jax.random.normal(key, shape, jnp.float32) * scale * gain
    return jnp.minimum(jnp.maximum(values, -limit), limit).astype(dtype)


def setup_inputs(seed: int = 0, part: int = 0) -> dict:
    seeds = jax.random.split(jax.random.key(seed), 8)
    part_keys = jax.random.split(jax.random.fold_in(seeds[7], part), 8)
    tokens = scatter_about(part_keys[0], (TOKENS, D), 1.0, 6.0, ((0, 32),))
    pre_gain = jnp.clip(1.0 + 0.18 * jax.random.normal(seeds[1], (D,), jnp.float32), 0.1, 1.9)
    up_weight = scatter_about(seeds[2], (D, FF), D ** -0.5, 0.125, ((0, 32), (1, 8)), jnp.float32)
    up_scale = jnp.clip(jnp.exp(math.log(3.0) - 2.3025851 * jax.random.uniform(seeds[3], (FF,), jnp.float32) ** levels(seeds[3], (FF,), ((0, 8),), -0.2, 0.2)), 0.3, 3.0)
    down_weight = scatter_about(seeds[4], (FF, D), FF ** -0.5, 0.0625, ((0, 8), (1, 32)), jnp.float32)
    down_scale = jnp.clip(jnp.exp(math.log(3.0) - 2.3025851 * jax.random.uniform(seeds[5], (D,), jnp.float32) ** levels(seeds[5], (D,), ((0, 32),), -0.2, 0.2)), 0.3, 3.0)
    post_gain = jnp.clip(1.0 + 0.18 * jax.random.normal(seeds[6], (D,), jnp.float32), 0.1, 1.9)
    return {"tokens": tokens, "pre_gain": pre_gain, "up_weight": up_weight, "up_scale": up_scale, "down_weight": down_weight, "down_scale": down_scale, "post_gain": post_gain}


epsilon = 1e-06

def rms_rows(values, scaling):
    return values * lax.rsqrt(lax.optimization_barrier(jnp.mean(values * values, axis=-1, keepdims=True)) + epsilon) * scaling

def reference(tokens, pre_gain, up_weight, up_scale, down_weight, down_scale, post_gain):
    up_cast = up_weight.astype(jnp.bfloat16)
    down_cast = down_weight.astype(jnp.bfloat16)
    block_width = FF // N_TP

    def row_block(rows):
        residual = rows.astype(jnp.float32)
        normed = rms_rows(residual, pre_gain).astype(jnp.bfloat16)
        lifted = jnp.dot(normed, up_cast, preferred_element_type=jnp.float32) * up_scale
        hidden = jnp.square(jax.nn.relu(lifted)).astype(jnp.bfloat16)
        running = jnp.zeros((rows.shape[0], D), jnp.float32)
        for member in range(N_TP):
            low = member * block_width
            high = low + block_width
            partial_value = jnp.dot(hidden[:, low:high], down_cast[low:high], preferred_element_type=jnp.float32) * down_scale
            partial_value = lax.optimization_barrier(partial_value.astype(jnp.bfloat16))
            running = running + partial_value.astype(jnp.float32)
        branch = lax.optimization_barrier(running.astype(jnp.bfloat16)).astype(jnp.float32)
        return (residual + rms_rows(branch, post_gain)).astype(jnp.bfloat16)
    result = lax.map(row_block, tokens.reshape(N_FS, TOK_DEV, D))
    return result.reshape(N_FS * TOK_DEV, D)
```

```python
import functools

import jax
import jax.numpy as jnp
from jax import lax
from jax.experimental import pallas as pl
from jax.experimental.pallas import tpu as pltpu
from jax.sharding import PartitionSpec as P

epsilon = 1e-06
MESH = pl.DeviceIdType.MESH

LAG = 8
PER = 2
UP_PARTS = 2
TOKEN_PARTS = 4


def remote(src, dst, send_sem, recv_sem, **where):
    return pltpu.make_async_remote_copy(
        src_ref=src, dst_ref=dst, send_sem=send_sem, recv_sem=recv_sem, device_id=where, device_id_type=MESH
    )


def arrived(ref, sem):
    pltpu.make_async_copy(ref, ref, sem).wait()


def kernel(
    nz, nx, tok, gain, upb, dnb, post, out,
    up, down, other, normed, acc, hidden, part, ypart, xpart, branch,
    up_in, down_in, up_sib, down_sib, tok_in, y_in, x_in, all_in, branch_sib,
    up_out, down_out, up_sib_out, down_sib_out, tok_out, y_out, x_out, all_out, all_sib_out,
):
    half = nz // 2
    rows, width = tok.shape
    block = width // nz
    quad = 4 * block
    n_quads = width // quad
    own = rows // nx
    tok_rows = rows // TOKEN_PARTS

    g = lax.axis_index("grp")
    z = lax.axis_index("fs")
    t = lax.axis_index("tp")
    y = lax.rem(g, 2)
    c = lax.rem(t, 2)
    x = t // 2
    partner = g + 1 - 2 * y
    sibling = t + 1 - 2 * c
    right = lax.rem(z + 1, nz)
    left = lax.rem(z + nz - 1, nz)
    home = c == y
    z_quad = z // 4

    def peer(i):
        return lax.rem(x + i, nx)

    barrier = pltpu.get_barrier_semaphore()
    neighbours = [{"fs": left}, {"fs": right}, {"tp": sibling}, {"grp": partner}]
    neighbours += [{"tp": 2 * peer(i) + c} for i in range(1, nx)]
    for where in neighbours:
        pl.semaphore_signal(barrier, inc=1, device_id=where, device_id_type=MESH)
    pl.semaphore_wait(barrier, len(neighbours))

    def quad_of(j):
        step = (j + 1) // 2
        return lax.rem(z_quad + n_quads + jnp.where(lax.rem(j, 2) == 1, -step, step), n_quads)

    def at_block(buf, b, k=0, parts=1):
        piece = block // parts
        return buf.at[c, pl.ds(pl.multiple_of(b * block + k * piece, piece), piece)]

    def begin(src, buf, in_sem, sib_sem, out_sem, sib_out, parts):
        piece = block // parts
        for k in range(parts):
            view = src.at[pl.ds(k * piece, piece)]
            for there in (right, left):
                remote(view, at_block(buf, z, k, parts), out_sem, in_sem.at[z * parts + k], fs=there).start()
        remote(src, at_block(buf, z), sib_out, sib_sem.at[0], tp=sibling).start()

    def ring_step(s, buf, in_sem, sib_sem, out_sem, sib_out, parts):
        back = lax.rem(z + nz - s, nz)
        ahead = lax.rem(z + s, nz)
        for k in range(parts):
            view = at_block(buf, back, k, parts)
            sem = in_sem.at[back * parts + k]
            arrived(view, sem)

            @pl.when(s < half)
            def _():
                remote(view, view, out_sem, sem, fs=right).start()

            @pl.when(s < half)
            def _():
                view = at_block(buf, ahead, k, parts)
                sem = in_sem.at[ahead * parts + k]
                arrived(view, sem)

                @pl.when(s < half - 1)
                def _():
                    remote(view, view, out_sem, sem, fs=left).start()

        view = at_block(buf, back)
        remote(view, view, sib_out, sib_sem.at[s // 4], tp=sibling).start()

        @pl.when(s < half)
        def _():
            view = at_block(buf, ahead)
            remote(view, view, sib_out, sib_sem.at[s // 4], tp=sibling).start()

    def from_sibling(j, buf, sib_sem):
        @pl.when(j == 0)
        def _():
            arrived(buf.at[1 - c, pl.ds(0, 7 * block)], sib_sem.at[0])

        @pl.when((lax.rem(j, 2) == 1) & (j < n_quads - 1))
        def _():
            arrived(buf.at[1 - c, pl.ds(0, 8 * block)], sib_sem.at[(j + 1) // 2])

        @pl.when(j == n_quads - 1)
        def _():
            arrived(buf.at[1 - c, pl.ds(0, block)], sib_sem.at[n_quads // 2])

    up_args = (up, up_in, up_sib, up_out, up_sib_out, UP_PARTS)
    down_args = (down, down_in, down_sib, down_out, down_sib_out, 1)
    begin(upb, *up_args)

    @pl.when(home)
    def _():
        for k in range(TOKEN_PARTS):
            view = pl.ds(k * tok_rows, tok_rows)
            remote(tok.at[view], other.at[view], tok_out, tok_in.at[k], grp=partner).start()

    begin(dnb, *down_args)
    up[c, pl.ds(pl.multiple_of(z * block, block), block), :] = upb[...]
    down[c, pl.ds(pl.multiple_of(z * block, block), block), :] = dnb[...]
    acc[...] = jnp.zeros_like(acc)

    def normalize(k):
        step = 32

        def from_rows(src):
            def body(i, _):
                view = pl.ds(pl.multiple_of(k * tok_rows + i * step, step), step)
                values = src[view, :].astype(jnp.float32)
                mean = jnp.mean(values * values, axis=-1, keepdims=True)
                scaled = (values * lax.rsqrt(mean + epsilon) * gain[...]).astype(jnp.bfloat16)
                for q in range(n_quads):
                    normed[q, view, :] = scaled[:, q * quad : (q + 1) * quad]
                return 0

            lax.fori_loop(0, tok_rows // step, body, 0)

        @pl.when(home)
        def _():
            from_rows(tok)

        @pl.when(jnp.logical_not(home))
        def _():
            view = pl.ds(pl.multiple_of(k * tok_rows, tok_rows), tok_rows)
            arrived(other.at[view], tok_in.at[k])
            from_rows(other)

    def lift(j):
        from_sibling(j, up, up_sib)
        q = quad_of(j)
        view = pl.ds(pl.multiple_of(q * quad, quad), quad)
        for h in range(2):
            acc[h] += jnp.dot(normed[q], up[h, view, :], preferred_element_type=jnp.float32)

    first = 10

    def up_pass(s, _):
        ring_step(s, *up_args)

        @pl.when(s > LAG)
        def _():
            ring_step(s - LAG, *down_args)

        @pl.when((lax.rem(s, 2) == 1) & (s >= 3) & (s < 3 + 2 * TOKEN_PARTS))
        def _():
            normalize((s - 3) // 2)

        @pl.when((s >= first) & (s < half))
        def _():
            lift(s - first)

        return 0

    lax.fori_loop(1, half + 1, up_pass, 0)

    def lift_rest(j, _):
        lift(j)
        return 0

    lax.fori_loop(half - first, n_quads, lift_rest, 0)
    for h in range(2):
        hidden[h] = jnp.square(jnp.maximum(acc[h], 0.0)).astype(jnp.bfloat16)

    own_rows = pl.ds(pl.multiple_of(x * own, own), own)

    def project(j):
        from_sibling(j, down, down_sib)
        q = quad_of(j)
        view = pl.ds(pl.multiple_of(q * quad, quad), quad)
        total = None
        for h in range(2):
            term = lax.dot_general(
                hidden[h], down[h, view, :], (((1,), (1,)), ((), ())), preferred_element_type=jnp.float32
            )
            total = term if total is None else total + term
        part[j] = total.astype(jnp.bfloat16)

        @pl.when(jnp.logical_not(home))
        def _():
            remote(part.at[j], ypart.at[j], y_out, y_in.at[j], grp=partner).start()

    def pair_sum(j):
        arrived(ypart.at[j], y_in.at[j])
        part[j] = (part[j].astype(jnp.float32) + ypart[j].astype(jnp.float32)).astype(jnp.bfloat16)
        for i in range(1, nx):
            view = pl.ds(pl.multiple_of(peer(i) * own, own), own)
            slot = nx - 1 - i
            remote(
                part.at[j, view], xpart.at[slot, j], x_out, x_in.at[slot * n_quads + j], tp=2 * peer(i) + c
            ).start()

    def row_sum(j):
        q = quad_of(j)
        total = part[j, own_rows, :].astype(jnp.float32)
        for i in range(nx - 1):
            arrived(xpart.at[i, j], x_in.at[i * n_quads + j])
            total += xpart[i, j].astype(jnp.float32)
        branch[q, own_rows, :] = total.astype(jnp.bfloat16)
        view = branch.at[q, own_rows]
        for i in range(1, nx):
            slot = nx - 1 - i
            remote(view, view, all_out, all_in.at[slot * n_quads + j], tp=2 * peer(i) + c).start()
        remote(view, view, all_sib_out, branch_sib, tp=sibling).start()

    def hand_on(j):
        q = quad_of(j)
        for i in range(1, nx):
            view = branch.at[q, pl.ds(pl.multiple_of(peer(i) * own, own), own)]
            arrived(view, all_in.at[(i - 1) * n_quads + j])
            remote(view, view, all_sib_out, branch_sib, tp=sibling).start()

    def output_pass(i, _):
        done = half - LAG + PER * i

        def more(s, _):
            ring_step(s, *down_args)
            return 0

        lax.fori_loop(jnp.minimum(done, half) + 1, jnp.minimum(done + PER, half) + 1, more, 0)

        @pl.when(i < n_quads)
        def _():
            project(i)

        @pl.when(home)
        def _():
            for behind, stage in ((1, pair_sum), (2, row_sum), (3, hand_on)):

                @pl.when((i >= behind) & (i < n_quads + behind))
                def _():
                    stage(i - behind)

        return 0

    lax.fori_loop(0, n_quads + 3, output_pass, 0)

    sent = (nz - 1) * block
    for buf, out_sem, sib_out in ((up, up_out, up_sib_out), (down, down_out, down_sib_out)):
        arrived(buf.at[0, pl.ds(0, sent)], out_sem)
        arrived(buf.at[0], sib_out)

    @pl.when(home)
    def _():
        arrived(tok, tok_out)
        most = part.at[pl.ds(0, n_quads * (nx - 1) // nx)]
        arrived(most, x_out)
        arrived(most, all_out)
        arrived(part, all_sib_out)

    @pl.when(jnp.logical_not(home))
    def _():
        arrived(part, y_out)
        arrived(branch, branch_sib)

    step = 32

    def finish(i, _):
        view = pl.ds(pl.multiple_of(i * step, step), step)
        squares = jnp.zeros((step, 1), jnp.float32)
        for q in range(n_quads):
            values = branch[q, view, :].astype(jnp.float32)
            squares += jnp.sum(values * values, axis=-1, keepdims=True)
        scale = lax.rsqrt(squares / width + epsilon)
        for q in range(n_quads):
            cols = slice(q * quad, (q + 1) * quad)
            values = branch[q, view, :].astype(jnp.float32)
            result = tok[view, cols].astype(jnp.float32) + values * scale * post[:, cols]
            out[view, cols] = result.astype(jnp.bfloat16)
        return 0

    lax.fori_loop(0, rows // step, finish, 0)


def solution(mesh):
    nz, nx = mesh.shape["fs"], mesh.shape["tp"] // 2

    def on_device(tokens, pre_gain, up_weight, up_scale, down_weight, down_scale, post_gain):
        rows, width = tokens.shape
        block, units = up_weight.shape
        mine = units // 2
        offset = lax.rem(lax.axis_index("grp"), 2) * mine
        upb = lax.dynamic_slice_in_dim(up_weight * up_scale, offset, mine, 1).astype(jnp.bfloat16)
        dnb = lax.dynamic_slice_in_dim(down_weight, offset, mine, 0) * down_scale
        dnb = dnb.T.astype(jnp.bfloat16)
        quad = 4 * block
        n_quads = width // quad
        own = rows // nx
        vmem = pl.BlockSpec(memory_space=pltpu.VMEM)
        bf16, f32 = jnp.bfloat16, jnp.float32
        dma = pltpu.SemaphoreType.DMA
        return pl.pallas_call(
            functools.partial(kernel, nz, nx),
            out_shape=jax.ShapeDtypeStruct((rows, width), bf16),
            in_specs=[vmem] * 5,
            out_specs=vmem,
            scratch_shapes=[
                pltpu.VMEM((2, width, mine), bf16),
                pltpu.VMEM((2, width, mine), bf16),
                pltpu.VMEM((rows, width), bf16),
                pltpu.VMEM((n_quads, rows, quad), bf16),
                pltpu.VMEM((2, rows, mine), f32),
                pltpu.VMEM((2, rows, mine), bf16),
                pltpu.VMEM((n_quads, rows, quad), bf16),
                pltpu.VMEM((n_quads, rows, quad), bf16),
                pltpu.VMEM((nx - 1, n_quads, own, quad), bf16),
                pltpu.VMEM((n_quads, rows, quad), bf16),
                dma((nz * UP_PARTS,)),
                dma((nz,)),
                dma((nz // 8 + 1,)),
                dma((nz // 8 + 1,)),
                dma((TOKEN_PARTS,)),
                dma((n_quads,)),
                dma(((nx - 1) * n_quads,)),
                dma(((nx - 1) * n_quads,)),
                dma,
                dma,
                dma,
                dma,
                dma,
                dma,
                dma,
                dma,
                dma,
                dma,
            ],
            compiler_params=pltpu.CompilerParams(
                collective_id=0, has_side_effects=True, vmem_limit_bytes=60 * 1024 * 1024
            ),
        )(tokens, pre_gain.reshape(1, width), upb, dnb, post_gain.reshape(1, width))

    placed = (P(("grp", "fs"), None), P(), P("fs", "tp"), P("tp"), P("tp", "fs"), P("fs"), P())
    return jax.shard_map(
        on_device, mesh=mesh, in_specs=placed, out_specs=P(("grp", "fs"), None), check_vma=False
    )
```

```python
import functools

import jax
import jax.numpy as jnp
from jax import lax
from jax.experimental import pallas as pl
from jax.experimental.pallas import tpu as pltpu
from jax.sharding import PartitionSpec as P

epsilon = 1e-06
MESH = pl.DeviceIdType.MESH

LAG = 6
PER = 2
PARTS = 2
TOKEN_PARTS = 4
ORDER = (1, 2, 0, 3, 7, 4, 6, 5)


def remote(src, dst, send_sem, recv_sem, **where):
    return pltpu.make_async_remote_copy(
        src_ref=src, dst_ref=dst, send_sem=send_sem, recv_sem=recv_sem, device_id=where, device_id_type=MESH
    )


def arrived(ref, sem):
    pltpu.make_async_copy(ref, ref, sem).wait()


def kernel(
    nz, nx, tok, gain, up_w, up_s, down_w, down_s, post, out,
    up, down, other, normed, acc, hidden, part, ypart, xpart, branch,
    up_in, down_in, up_sib, down_sib, tok_in, y_in, x_in, all_in, branch_sib,
    up_out, down_out, up_sib_out, down_sib_out, own_sib_out, tok_out, y_out, x_out, all_out, all_sib_out,
):
    rows, width = tok.shape
    block, units = up_w.shape
    mine = units // 2
    quad = 4 * block
    n_quads = width // quad
    own = rows // nx
    tok_rows = rows // TOKEN_PARTS
    piece = block // PARTS
    reach = (nz * 13 // 32, nz - 1 - nz * 13 // 32)

    g = lax.axis_index("grp")
    z = lax.axis_index("fs")
    t = lax.axis_index("tp")
    y = lax.rem(g, 2)
    c = lax.rem(t, 2)
    x = t // 2
    partner = g + 1 - 2 * y
    sibling = t + 1 - 2 * c
    way = 1 - 2 * c
    following = lax.rem(z + way + nz, nz)
    previous = lax.rem(z - way + nz, nz)
    home = c == y
    z_quad = z // 4
    last = jnp.where(c == 0, reach[0], reach[1])

    def peer(i):
        return lax.rem(x + i, nx)

    barrier = pltpu.get_barrier_semaphore()
    neighbours = [{"fs": previous}, {"tp": sibling}, {"grp": partner}]
    neighbours += [{"tp": 2 * peer(i) + c} for i in range(1, nx)]
    for where in neighbours:
        pl.semaphore_signal(barrier, inc=1, device_id=where, device_id_type=MESH)

    half = pl.ds(pl.multiple_of(y * mine, mine), mine)
    up[z, c] = (up_w[:, half] * up_s[:, half]).astype(jnp.bfloat16)
    line = lax.broadcasted_iota(jnp.int32, (block, block), 0) == lax.broadcasted_iota(jnp.int32, (block, block), 1)
    column = jnp.sum(jnp.where(line, jnp.broadcast_to(down_s[...], (block, block)), 0.0), axis=1, keepdims=True)
    down[z, c] = (down_w[:, half] * column).astype(jnp.bfloat16)
    acc[...] = jnp.zeros_like(acc)
    pl.semaphore_wait(barrier, len(neighbours))

    def quad_of(j):
        return lax.rem(z_quad + sum(jnp.where(j == k, ORDER[k], 0) for k in range(n_quads)), n_quads)

    def send_half(b, h, buf, in_sem, out_sem, wait):
        for k in range(PARTS):
            view = buf.at[b, h, pl.ds(k * piece, piece)]
            sem = in_sem.at[(2 * b + h) * PARTS + k]
            if wait is not None:
                arrived(view, sem)

            @pl.when(True if wait is None else wait)
            def _():
                remote(view, view, out_sem, sem, fs=following).start()

    def begin(buf, in_sem, sib_sem, out_sem, sib_out):
        send_half(z, c, buf, in_sem, out_sem, None)
        arrived(buf.at[z, 1 - c], sib_sem.at[z])
        send_half(z, 1 - c, buf, in_sem, out_sem, None)

    def ring_step(s, buf, in_sem, sib_sem, out_sem, sib_out):
        b = lax.rem(z - way * s + nz, nz)
        for h in (c, 1 - c):
            send_half(b, h, buf, in_sem, out_sem, s < last)
        remote(buf.at[b], buf.at[b], sib_out, sib_sem.at[b], tp=sibling).start()

    def from_sibling(q, buf, sib_sem):
        for i in range(4):
            b = 4 * q + i
            ahead = lax.rem(b - z + nz, nz)

            @pl.when((ahead > 0) & jnp.where(c == 0, ahead <= reach[1], ahead > reach[1]))
            def _():
                arrived(buf.at[b], sib_sem.at[b])

    up_args = (up, up_in, up_sib, up_out, up_sib_out)
    down_args = (down, down_in, down_sib, down_out, down_sib_out)
    for buf, sib_sem in ((up, up_sib), (down, down_sib)):
        remote(buf.at[z, c], buf.at[z, c], own_sib_out, sib_sem.at[z], tp=sibling).start()
    begin(*up_args)

    @pl.when(home)
    def _():
        for k in range(TOKEN_PARTS):
            view = pl.ds(k * tok_rows, tok_rows)
            remote(tok.at[view], other.at[view], tok_out, tok_in.at[k], grp=partner).start()

    def normalize(k):
        step = 32

        def from_rows(src):
            def body(i, _):
                view = pl.ds(pl.multiple_of(k * tok_rows + i * step, step), step)
                values = src[view, :].astype(jnp.float32)
                mean = jnp.mean(values * values, axis=-1, keepdims=True)
                scaled = (values * lax.rsqrt(mean + epsilon) * gain[...]).astype(jnp.bfloat16)
                for q in range(n_quads):
                    normed[q, view, :] = scaled[:, q * quad : (q + 1) * quad]
                return 0

            lax.fori_loop(0, tok_rows // step, body, 0)

        @pl.when(home)
        def _():
            from_rows(tok)

        @pl.when(jnp.logical_not(home))
        def _():
            view = pl.ds(pl.multiple_of(k * tok_rows, tok_rows), tok_rows)
            arrived(other.at[view], tok_in.at[k])
            from_rows(other)

    def lift(m):
        q = lax.rem(z_quad - way * m + n_quads + 8, n_quads)
        from_sibling(q, up, up_sib)
        for h in range(2):
            weights = up[pl.ds(4 * q, 4), h].reshape(quad, mine)
            acc[h] += jnp.dot(normed[q], weights, preferred_element_type=jnp.float32)

    norm_at = 8
    lift_at = norm_at + TOKEN_PARTS

    def up_pass(s, _):
        ring_step(s, *up_args)

        @pl.when(s == LAG)
        def _():
            begin(*down_args)

        @pl.when(s > LAG)
        def _():
            ring_step(s - LAG, *down_args)

        @pl.when((s >= norm_at) & (s < lift_at))
        def _():
            normalize(s - norm_at)

        @pl.when((s == lift_at) | (s == lift_at + 1) | (s == lift_at + 4))
        def _():
            lift(jnp.minimum(s - lift_at + 1, 3))

        return 0

    lax.fori_loop(1, last + 1, up_pass, 0)

    def lift_rest(m, _):
        lift(m)
        return 0

    lax.fori_loop(jnp.where(c == 0, 3, 4), n_quads + 1, lift_rest, 0)
    for h in range(2):
        hidden[h] = jnp.square(jnp.maximum(acc[h], 0.0)).astype(jnp.bfloat16)

    own_rows = pl.ds(pl.multiple_of(x * own, own), own)

    def project(j):
        q = quad_of(j)
        from_sibling(q, down, down_sib)
        total = None
        for h in range(2):
            weights = down[pl.ds(4 * q, 4), h].reshape(quad, mine)
            term = lax.dot_general(
                hidden[h], weights, (((1,), (1,)), ((), ())), preferred_element_type=jnp.float32
            )
            total = term if total is None else total + term
        part[j] = total.astype(jnp.bfloat16)

        @pl.when(jnp.logical_not(home))
        def _():
            remote(part.at[j], ypart.at[j], y_out, y_in.at[j], grp=partner).start()

    def pair_sum(j):
        arrived(ypart.at[j], y_in.at[j])
        part[j] = (part[j].astype(jnp.float32) + ypart[j].astype(jnp.float32)).astype(jnp.bfloat16)
        for i in range(1, nx):
            view = pl.ds(pl.multiple_of(peer(i) * own, own), own)
            slot = nx - 1 - i
            remote(
                part.at[j, view], xpart.at[slot, j], x_out, x_in.at[slot * n_quads + j], tp=2 * peer(i) + c
            ).start()

    def row_sum(j):
        q = quad_of(j)
        total = part[j, own_rows, :].astype(jnp.float32)
        for i in range(nx - 1):
            arrived(xpart.at[i, j], x_in.at[i * n_quads + j])
            total += xpart[i, j].astype(jnp.float32)
        branch[q, own_rows, :] = total.astype(jnp.bfloat16)
        view = branch.at[q, own_rows]
        for i in (1, nx - 1):
            remote(view, view, all_out, all_in.at[(nx - 1 - i) * n_quads + j], tp=2 * peer(i) + c).start()
        remote(view, view, all_sib_out, branch_sib, tp=sibling).start()

    def take(i, j):
        view = branch.at[quad_of(j), pl.ds(pl.multiple_of(peer(i) * own, own), own)]
        arrived(view, all_in.at[(i - 1) * n_quads + j])
        remote(view, view, all_sib_out, branch_sib, tp=sibling).start()
        return view

    def hand_on(j):
        view = take(1, j)
        remote(view, view, all_out, all_in.at[n_quads + j], tp=2 * peer(nx - 1) + c).start()
        take(nx - 1, j)

    def hand_far(j):
        take(2, j)

    def output_pass(i, _):
        done = last - LAG + PER * i

        def more(s, _):
            ring_step(s, *down_args)
            return 0

        lax.fori_loop(jnp.minimum(done, last) + 1, jnp.minimum(done + PER, last) + 1, more, 0)

        @pl.when(i < n_quads)
        def _():
            project(i)

        @pl.when(home)
        def _():
            for behind, stage in ((1, pair_sum), (2, row_sum), (3, hand_on), (4, hand_far)):

                @pl.when((i >= behind) & (i < n_quads + behind))
                def _():
                    stage(i - behind)

        return 0

    lax.fori_loop(0, n_quads + 4, output_pass, 0)

    for side in range(2):

        @pl.when(c == side)
        def _():
            for sem in (up_out, down_out, up_sib_out, down_sib_out):
                arrived(up.at[pl.ds(0, reach[side])], sem)

    arrived(up.at[0], own_sib_out)

    @pl.when(home)
    def _():
        arrived(tok, tok_out)
        most = part.at[pl.ds(0, n_quads * (nx - 1) // nx)]
        arrived(most, x_out)
        arrived(most, all_out)
        arrived(part, all_sib_out)

    @pl.when(jnp.logical_not(home))
    def _():
        arrived(part, y_out)
        arrived(branch, branch_sib)

    step = 32

    def finish(i, _):
        view = pl.ds(pl.multiple_of(i * step, step), step)
        squares = jnp.zeros((step, 1), jnp.float32)
        for q in range(n_quads):
            values = branch[q, view, :].astype(jnp.float32)
            squares += jnp.sum(values * values, axis=-1, keepdims=True)
        scale = lax.rsqrt(squares / width + epsilon)
        for q in range(n_quads):
            cols = slice(q * quad, (q + 1) * quad)
            values = branch[q, view, :].astype(jnp.float32)
            result = tok[view, cols].astype(jnp.float32) + values * scale * post[:, cols]
            out[view, cols] = result.astype(jnp.bfloat16)
        return 0

    lax.fori_loop(0, rows // step, finish, 0)


def solution(mesh):
    nz, nx = mesh.shape["fs"], mesh.shape["tp"] // 2

    def on_device(tokens, pre_gain, up_weight, up_scale, down_weight, down_scale, post_gain):
        rows, width = tokens.shape
        block, units = up_weight.shape
        mine = units // 2
        quad = 4 * block
        n_quads = width // quad
        own = rows // nx
        vmem = pl.BlockSpec(memory_space=pltpu.VMEM)
        bf16, f32 = jnp.bfloat16, jnp.float32
        dma = pltpu.SemaphoreType.DMA
        return pl.pallas_call(
            functools.partial(kernel, nz, nx),
            out_shape=jax.ShapeDtypeStruct((rows, width), bf16),
            in_specs=[vmem] * 7,
            out_specs=vmem,
            scratch_shapes=[
                pltpu.VMEM((nz, 2, block, mine), bf16),
                pltpu.VMEM((nz, 2, block, mine), bf16),
                pltpu.VMEM((rows, width), bf16),
                pltpu.VMEM((n_quads, rows, quad), bf16),
                pltpu.VMEM((2, rows, mine), f32),
                pltpu.VMEM((2, rows, mine), bf16),
                pltpu.VMEM((n_quads, rows, quad), bf16),
                pltpu.VMEM((n_quads, rows, quad), bf16),
                pltpu.VMEM((nx - 1, n_quads, own, quad), bf16),
                pltpu.VMEM((n_quads, rows, quad), bf16),
                dma((nz * 2 * PARTS,)),
                dma((nz * 2 * PARTS,)),
                dma((nz,)),
                dma((nz,)),
                dma((TOKEN_PARTS,)),
                dma((n_quads,)),
                dma(((nx - 1) * n_quads,)),
                dma(((nx - 1) * n_quads,)),
                dma,
                dma,
                dma,
                dma,
                dma,
                dma,
                dma,
                dma,
                dma,
                dma,
                dma,
            ],
            compiler_params=pltpu.CompilerParams(
                collective_id=0, has_side_effects=True, vmem_limit_bytes=60 * 1024 * 1024
            ),
        )(
            tokens,
            pre_gain.reshape(1, width),
            up_weight,
            up_scale.reshape(1, units),
            down_weight.T,
            down_scale.reshape(1, block),
            post_gain.reshape(1, width),
        )

    placed = (P(("grp", "fs"), None), P(), P("fs", "tp"), P("tp"), P("tp", "fs"), P("fs"), P())
    return jax.shard_map(
        on_device, mesh=mesh, in_specs=placed, out_specs=P(("grp", "fs"), None), check_vma=False
    )
```

```python
import functools

import jax
import jax.numpy as jnp
from jax import lax
from jax.experimental import pallas as pl
from jax.experimental.pallas import tpu as pltpu
from jax.sharding import PartitionSpec as P

epsilon = 1e-06
MESH = pl.DeviceIdType.MESH

LAG = 2
PARTS = 2
TOKEN_PARTS = 4
ORDER = (1, 2, 0, 3, 7, 4, 6, 5)


def remote(src, dst, send_sem, recv_sem, **where):
    return pltpu.make_async_remote_copy(
        src_ref=src, dst_ref=dst, send_sem=send_sem, recv_sem=recv_sem, device_id=where, device_id_type=MESH
    )


def arrived(ref, sem):
    pltpu.make_async_copy(ref, ref, sem).wait()


def kernel(
    nz, nx, tok, gain, up_w, up_s, down_w, down_s, out,
    up, down, seen, normed, acc, hidden, part, ypart, xpart, branch,
    up_in, down_in, up_sib, down_sib, tok_in, y_in, x_in, all_in, branch_sib,
    up_out, down_out, up_sib_out, down_sib_out, own_sib_out, tok_out, y_out, x_out, all_out, all_sib_out, out_sem,
):
    rows, width = tok.shape
    block, units = up_w.shape
    mine = units // 2
    quad = 4 * block
    n_quads = width // quad
    own = rows // nx
    tok_rows = rows // TOKEN_PARTS
    piece = block // PARTS
    reach = (nz * 13 // 32, nz - 1 - nz * 13 // 32)

    g = lax.axis_index("grp")
    z = lax.axis_index("fs")
    t = lax.axis_index("tp")
    y = lax.rem(g, 2)
    c = lax.rem(t, 2)
    x = t // 2
    partner = g + 1 - 2 * y
    sibling = t + 1 - 2 * c
    way = 1 - 2 * c
    following = lax.rem(z + way + nz, nz)
    previous = lax.rem(z - way + nz, nz)
    home = c == y
    z_quad = z // 4
    last = jnp.where(c == 0, reach[0], reach[1])

    def peer(i):
        return lax.rem(x + i, nx)

    barrier = pltpu.get_barrier_semaphore()
    neighbours = [{"fs": previous}, {"tp": sibling}, {"grp": partner}]
    neighbours += [{"tp": 2 * peer(i) + c} for i in range(1, nx)]
    for where in neighbours:
        pl.semaphore_signal(barrier, inc=1, device_id=where, device_id_type=MESH)

    def token_rows(k):
        return pl.ds(pl.multiple_of(k * tok_rows, tok_rows), tok_rows)

    @pl.when(home)
    def _():
        for k in range(TOKEN_PARTS):
            pltpu.make_async_copy(tok.at[token_rows(k)], seen.at[token_rows(k)], tok_in.at[k]).start()

    half = pl.ds(pl.multiple_of(y * mine, mine), mine)
    up[z, c] = (up_w[:, half] * up_s[:, half]).astype(jnp.bfloat16)
    line = lax.broadcasted_iota(jnp.int32, (block, block), 0) == lax.broadcasted_iota(jnp.int32, (block, block), 1)
    column = jnp.sum(jnp.where(line, jnp.broadcast_to(down_s[...], (block, block)), 0.0), axis=1, keepdims=True)
    down[z, c] = (down_w[:, half] * column).astype(jnp.bfloat16)
    pl.semaphore_wait(barrier, len(neighbours))

    def quad_of(j):
        return lax.rem(z_quad + sum(jnp.where(j == k, ORDER[k], 0) for k in range(n_quads)), n_quads)

    def send_half(b, h, buf, in_sem, out_sem, wait):
        for k in range(PARTS):
            view = buf.at[b, h, pl.ds(k * piece, piece)]
            sem = in_sem.at[(2 * b + h) * PARTS + k]
            if wait is not None:
                arrived(view, sem)

            @pl.when(True if wait is None else wait)
            def _():
                remote(view, view, out_sem, sem, fs=following).start()

    def begin(buf, in_sem, sib_sem, out_sem, sib_out):
        send_half(z, c, buf, in_sem, out_sem, None)
        arrived(buf.at[z, 1 - c], sib_sem.at[z])
        send_half(z, 1 - c, buf, in_sem, out_sem, None)

    def ring_step(s, buf, in_sem, sib_sem, out_sem, sib_out):
        b = lax.rem(z - way * s + nz, nz)
        for h in (c, 1 - c):
            send_half(b, h, buf, in_sem, out_sem, s < last)
        remote(buf.at[b], buf.at[b], sib_out, sib_sem.at[b], tp=sibling).start()

    def from_sibling(q, buf, sib_sem):
        for i in range(4):
            b = 4 * q + i
            ahead = lax.rem(b - z + nz, nz)

            @pl.when((ahead > 0) & jnp.where(c == 0, ahead <= reach[1], ahead > reach[1]))
            def _():
                arrived(buf.at[b], sib_sem.at[b])

    up_args = (up, up_in, up_sib, up_out, up_sib_out)
    down_args = (down, down_in, down_sib, down_out, down_sib_out)
    for buf, sib_sem in ((up, up_sib), (down, down_sib)):
        remote(buf.at[z, c], buf.at[z, c], own_sib_out, sib_sem.at[z], tp=sibling).start()

    @pl.when(home)
    def _():
        for k in range(TOKEN_PARTS):
            remote(tok.at[token_rows(k)], seen.at[token_rows(k)], tok_out, tok_in.at[k], grp=partner).start()

    begin(*up_args)
    acc[...] = jnp.zeros_like(acc)

    def normalize(k):
        arrived(seen.at[token_rows(k)], tok_in.at[k])
        step = 32

        def body(i, _):
            view = pl.ds(pl.multiple_of(k * tok_rows + i * step, step), step)
            values = seen[view, :].astype(jnp.float32)
            mean = jnp.mean(values * values, axis=-1, keepdims=True)
            scaled = (values * lax.rsqrt(mean + epsilon) * gain[...]).astype(jnp.bfloat16)
            for q in range(n_quads):
                normed[q, view, :] = scaled[:, q * quad : (q + 1) * quad]
            return 0

        lax.fori_loop(0, tok_rows // step, body, 0)

    def lift(m):
        q = lax.rem(z_quad - way * m + n_quads + 8, n_quads)
        from_sibling(q, up, up_sib)
        for h in range(2):
            weights = up[pl.ds(4 * q, 4), h].reshape(quad, mine)
            acc[h] += jnp.dot(normed[q], weights, preferred_element_type=jnp.float32)

    norm_at = 8 + 4 * c
    lift_at = norm_at + TOKEN_PARTS

    def ring_pass(s, _):
        @pl.when(s <= last)
        def _():
            ring_step(s, *up_args)

        @pl.when(s == LAG)
        def _():
            begin(*down_args)

        @pl.when(s > LAG)
        def _():
            ring_step(s - LAG, *down_args)

        @pl.when((s >= norm_at) & (s < lift_at))
        def _():
            normalize(s - norm_at)

        @pl.when((s >= lift_at) & (s < lift_at + 2 + c))
        def _():
            lift(s - lift_at + 1)

        return 0

    lax.fori_loop(1, last + LAG + 1, ring_pass, 0)

    def lift_rest(m, _):
        lift(m)
        return 0

    lax.fori_loop(jnp.where(c == 0, 3, 4), n_quads + 1, lift_rest, 0)
    for h in range(2):
        hidden[h] = jnp.square(jnp.maximum(acc[h], 0.0)).astype(jnp.bfloat16)

    own_rows = pl.ds(pl.multiple_of(x * own, own), own)

    def project(j):
        q = quad_of(j)
        from_sibling(q, down, down_sib)
        total = None
        for h in range(2):
            weights = down[pl.ds(4 * q, 4), h].reshape(quad, mine)
            term = lax.dot_general(
                hidden[h], weights, (((1,), (1,)), ((), ())), preferred_element_type=jnp.float32
            )
            total = term if total is None else total + term
        part[j] = total.astype(jnp.bfloat16)

        @pl.when(jnp.logical_not(home))
        def _():
            remote(part.at[j], ypart.at[j], y_out, y_in.at[j], grp=partner).start()

    def pair_sum(j):
        arrived(ypart.at[j], y_in.at[j])
        part[j] = (part[j].astype(jnp.float32) + ypart[j].astype(jnp.float32)).astype(jnp.bfloat16)
        for i in range(1, nx):
            view = pl.ds(pl.multiple_of(peer(i) * own, own), own)
            slot = nx - 1 - i
            remote(
                part.at[j, view], xpart.at[slot, j], x_out, x_in.at[slot * n_quads + j], tp=2 * peer(i) + c
            ).start()

    def row_sum(j):
        q = quad_of(j)
        total = part[j, own_rows, :].astype(jnp.float32)
        for i in range(nx - 1):
            arrived(xpart.at[i, j], x_in.at[i * n_quads + j])
            total += xpart[i, j].astype(jnp.float32)
        branch[q, own_rows, :] = total.astype(jnp.bfloat16)
        view = branch.at[q, own_rows]
        for i in (1, nx - 1):
            remote(view, view, all_out, all_in.at[(nx - 1 - i) * n_quads + j], tp=2 * peer(i) + c).start()
        remote(view, view, all_sib_out, branch_sib.at[j], tp=sibling).start()

    def take(i, j):
        view = branch.at[quad_of(j), pl.ds(pl.multiple_of(peer(i) * own, own), own)]
        arrived(view, all_in.at[(i - 1) * n_quads + j])
        remote(view, view, all_sib_out, branch_sib.at[j], tp=sibling).start()
        return view

    def hand_on(j):
        view = take(1, j)
        remote(view, view, all_out, all_in.at[n_quads + j], tp=2 * peer(nx - 1) + c).start()
        take(nx - 1, j)

    def hand_far(j):
        take(2, j)
        q = quad_of(j)
        pltpu.make_async_copy(branch.at[q], out.at[q], out_sem.at[j]).start()

    def output_pass(i, _):
        @pl.when(i < n_quads)
        def _():
            project(i)

        @pl.when(home)
        def _():
            for behind, stage in ((1, pair_sum), (2, row_sum), (3, hand_on), (4, hand_far)):

                @pl.when((i >= behind) & (i < n_quads + behind))
                def _():
                    stage(i - behind)

        return 0

    lax.fori_loop(0, n_quads + 4, output_pass, 0)

    for side in range(2):

        @pl.when(c == side)
        def _():
            for sem in (up_out, down_out, up_sib_out, down_sib_out):
                arrived(up.at[pl.ds(0, reach[side])], sem)

    arrived(up.at[0], own_sib_out)

    @pl.when(home)
    def _():
        arrived(seen, tok_out)
        most = part.at[pl.ds(0, n_quads * (nx - 1) // nx)]
        arrived(most, x_out)
        arrived(most, all_out)
        arrived(part, all_sib_out)

    @pl.when(jnp.logical_not(home))
    def _():
        arrived(part, y_out)
        for j in range(n_quads):
            q = quad_of(j)
            arrived(branch.at[q], branch_sib.at[j])
            pltpu.make_async_copy(branch.at[q], out.at[q], out_sem.at[j]).start()

    for j in range(n_quads):
        arrived(part.at[j], out_sem.at[j])


def finish(branch, tok, post, out):
    n_quads, _, quad = branch.shape
    values = branch[...].astype(jnp.float32)
    squares = jnp.sum(jnp.sum(values * values, axis=0), axis=-1, keepdims=True)
    scale = lax.rsqrt(squares / (n_quads * quad) + epsilon)
    for q in range(n_quads):
        cols = slice(q * quad, (q + 1) * quad)
        result = tok[:, cols].astype(jnp.float32) + values[q] * scale * post[:, cols]
        out[:, cols] = result.astype(jnp.bfloat16)


def solution(mesh):
    nz, nx = mesh.shape["fs"], mesh.shape["tp"] // 2

    def on_device(tokens, pre_gain, up_weight, up_scale, down_weight, down_scale, post_gain):
        rows, width = tokens.shape
        block, units = up_weight.shape
        mine = units // 2
        quad = 4 * block
        n_quads = width // quad
        own = rows // nx
        vmem = pl.BlockSpec(memory_space=pltpu.VMEM)
        bf16, f32 = jnp.bfloat16, jnp.float32
        dma = pltpu.SemaphoreType.DMA
        anywhere = pl.BlockSpec(memory_space=pl.ANY)
        branch = pl.pallas_call(
            functools.partial(kernel, nz, nx),
            out_shape=jax.ShapeDtypeStruct((n_quads, rows, quad), bf16),
            in_specs=[anywhere] + [vmem] * 5,
            out_specs=anywhere,
            scratch_shapes=[
                pltpu.VMEM((nz, 2, block, mine), bf16),
                pltpu.VMEM((nz, 2, block, mine), bf16),
                pltpu.VMEM((rows, width), bf16),
                pltpu.VMEM((n_quads, rows, quad), bf16),
                pltpu.VMEM((2, rows, mine), f32),
                pltpu.VMEM((2, rows, mine), bf16),
                pltpu.VMEM((n_quads, rows, quad), bf16),
                pltpu.VMEM((n_quads, rows, quad), bf16),
                pltpu.VMEM((nx - 1, n_quads, own, quad), bf16),
                pltpu.VMEM((n_quads, rows, quad), bf16),
                dma((nz * 2 * PARTS,)),
                dma((nz * 2 * PARTS,)),
                dma((nz,)),
                dma((nz,)),
                dma((TOKEN_PARTS,)),
                dma((n_quads,)),
                dma(((nx - 1) * n_quads,)),
                dma(((nx - 1) * n_quads,)),
                dma((n_quads,)),
                dma,
                dma,
                dma,
                dma,
                dma,
                dma,
                dma,
                dma,
                dma,
                dma,
                dma((n_quads,)),
            ],
            compiler_params=pltpu.CompilerParams(
                collective_id=0, has_side_effects=True, vmem_limit_bytes=60 * 1024 * 1024
            ),
        )(
            tokens,
            pre_gain.reshape(1, width),
            up_weight,
            up_scale.reshape(1, units),
            down_weight.T,
            down_scale.reshape(1, block),
        )
        step = rows // 4
        return pl.pallas_call(
            finish,
            grid=(rows // step,),
            out_shape=jax.ShapeDtypeStruct((rows, width), bf16),
            in_specs=[
                pl.BlockSpec((n_quads, step, quad), lambda i: (0, i, 0)),
                pl.BlockSpec((step, width), lambda i: (i, 0)),
                pl.BlockSpec((1, width), lambda i: (0, 0)),
            ],
            out_specs=pl.BlockSpec((step, width), lambda i: (i, 0)),
        )(branch, tokens, post_gain.reshape(1, width))

    placed = (P(("grp", "fs"), None), P(), P("fs", "tp"), P("tp"), P("tp", "fs"), P("fs"), P())
    return jax.shard_map(
        on_device, mesh=mesh, in_specs=placed, out_specs=P(("grp", "fs"), None), check_vma=False
    )
```

```python
import functools

import jax
import jax.numpy as jnp
from jax import lax
from jax.experimental import pallas as pl
from jax.experimental.pallas import tpu as pltpu
from jax.sharding import PartitionSpec as P

epsilon = 1e-06
MESH = pl.DeviceIdType.MESH

LAG = (8, 4)
PARTS = 4
TOKEN_PARTS = 4
LIFTS = ((1, 8, 2, 7, 6, 5, 3, 4), (1, 8, 2, 7, 3, 6, 5, 4))
ORDER = (1, 2, 0, 3, 7, 4, 6, 5)


def remote(src, dst, send_sem, recv_sem, **where):
    return pltpu.make_async_remote_copy(
        src_ref=src, dst_ref=dst, send_sem=send_sem, recv_sem=recv_sem, device_id=where, device_id_type=MESH
    )


def arrived(ref, sem):
    pltpu.make_async_copy(ref, ref, sem).wait()


def kernel(
    nz, nx, tok, gain, up_w, up_s, down_w, down_s, out,
    up, down, seen, normed, acc, hidden, part, ypart, xpart, branch,
    up_in, down_in, up_sib, down_sib, tok_in, y_in, x_in, all_in, branch_sib,
    up_out, down_out, up_sib_out, down_sib_out, own_sib_out, tok_out, y_out, x_out, all_out, all_sib_out, out_sem,
):
    rows, width = tok.shape
    block, units = up_w.shape
    mine = units // 2
    quad = 4 * block
    n_quads = width // quad
    n_chunks = 2 * n_quads
    tall = rows // 2
    own = tall // nx
    tok_rows = rows // TOKEN_PARTS
    piece = block // PARTS
    reach = (nz * 12 // 32, nz - 1 - nz * 12 // 32)

    g = lax.axis_index("grp")
    z = lax.axis_index("fs")
    t = lax.axis_index("tp")
    y = lax.rem(g, 2)
    c = lax.rem(t, 2)
    x = t // 2
    partner = g + 1 - 2 * y
    sibling = t + 1 - 2 * c
    way = 1 - 2 * c
    following = lax.rem(z + way + nz, nz)
    previous = lax.rem(z - way + nz, nz)
    home = c == y
    z_quad = z // 4
    last = jnp.where(c == 0, reach[0], reach[1])
    lag = jnp.where(c == 0, LAG[0], LAG[1])
    near = z < nz // 4

    def peer(i):
        return lax.rem(x + i, nx)

    barrier = pltpu.get_barrier_semaphore()
    neighbours = [{"fs": previous}, {"tp": sibling}, {"grp": partner}]
    neighbours += [{"tp": 2 * peer(i) + c} for i in range(1, nx)]
    for where in neighbours:
        pl.semaphore_signal(barrier, inc=1, device_id=where, device_id_type=MESH)

    def token_rows(k):
        return pl.ds(pl.multiple_of(k * tok_rows, tok_rows), tok_rows)

    @pl.when(home)
    def _():
        for k in range(TOKEN_PARTS):
            pltpu.make_async_copy(tok.at[token_rows(k)], seen.at[token_rows(k)], tok_in.at[k]).start()

    half = pl.ds(pl.multiple_of(y * mine, mine), mine)
    up[z, c] = (up_w[:, half] * up_s[:, half]).astype(jnp.bfloat16)
    line = lax.broadcasted_iota(jnp.int32, (block, block), 0) == lax.broadcasted_iota(jnp.int32, (block, block), 1)
    column = jnp.sum(jnp.where(line, jnp.broadcast_to(down_s[...], (block, block)), 0.0), axis=1, keepdims=True)
    down[z, c] = (down_w[:, half] * column).astype(jnp.bfloat16)
    pl.semaphore_wait(barrier, len(neighbours))

    def pick(values, i):
        return sum(jnp.where(i == k, v, 0) for k, v in enumerate(values))

    def quad_of(j):
        return lax.rem(z_quad + pick(ORDER, j // 2), n_quads)

    def chunk_rows(j, of=None):
        first = lax.rem(j, 2) * tall
        if of is None:
            return pl.ds(pl.multiple_of(first, tall), tall)
        return pl.ds(pl.multiple_of(first + of * own, own), own)

    def send_half(b, h, buf, in_sem, out_sem, wait):
        for k in range(PARTS):
            view = buf.at[b, h, pl.ds(k * piece, piece)]
            sem = in_sem.at[(2 * b + h) * PARTS + k]
            if wait is not None:
                arrived(view, sem)

            @pl.when(True if wait is None else wait)
            def _():
                remote(view, view, out_sem, sem, fs=following).start()

    def begin(buf, in_sem, sib_sem, out_sem, sib_out):
        send_half(z, c, buf, in_sem, out_sem, None)
        arrived(buf.at[z, 1 - c], sib_sem.at[z])
        send_half(z, 1 - c, buf, in_sem, out_sem, None)

    def ring_step(s, buf, in_sem, sib_sem, out_sem, sib_out):
        b = lax.rem(z - way * s + nz, nz)
        for h in (c, 1 - c):
            send_half(b, h, buf, in_sem, out_sem, s < last)
        remote(buf.at[b], buf.at[b], sib_out, sib_sem.at[b], tp=sibling).start()

    def from_sibling(q, buf, sib_sem):
        for i in range(4):
            b = 4 * q + i
            ahead = lax.rem(b - z + nz, nz)

            @pl.when((ahead > 0) & jnp.where(c == 0, ahead <= reach[1], ahead > reach[1]))
            def _():
                arrived(buf.at[b], sib_sem.at[b])

    up_args = (up, up_in, up_sib, up_out, up_sib_out)
    down_args = (down, down_in, down_sib, down_out, down_sib_out)
    for buf, sib_sem in ((up, up_sib), (down, down_sib)):
        remote(buf.at[z, c], buf.at[z, c], own_sib_out, sib_sem.at[z], tp=sibling).start()

    @pl.when(home)
    def _():
        for k in range(TOKEN_PARTS):
            remote(tok.at[token_rows(k)], seen.at[token_rows(k)], tok_out, tok_in.at[k], grp=partner).start()

    begin(*up_args)
    acc[...] = jnp.zeros_like(acc)

    def normalize(k):
        arrived(seen.at[token_rows(k)], tok_in.at[k])
        step = 32

        def body(i, _):
            view = pl.ds(pl.multiple_of(k * tok_rows + i * step, step), step)
            values = seen[view, :].astype(jnp.float32)
            mean = jnp.mean(values * values, axis=-1, keepdims=True)
            scaled = (values * lax.rsqrt(mean + epsilon) * gain[...]).astype(jnp.bfloat16)
            for q in range(n_quads):
                normed[q, view, :] = scaled[:, q * quad : (q + 1) * quad]
            return 0

        lax.fori_loop(0, tok_rows // step, body, 0)

    def lift(i, _):
        m = jnp.where(c == 0, pick(LIFTS[0], i), pick(LIFTS[1], i))
        q = lax.rem(z_quad - way * m + n_quads + 8, n_quads)
        from_sibling(q, up, up_sib)
        for h in range(2):
            weights = up[pl.ds(4 * q, 4), h].reshape(quad, mine)
            acc[h] += jnp.dot(normed[q], weights, preferred_element_type=jnp.float32)
        return 0

    def activate():
        for h in range(2):
            hidden[h] = jnp.square(jnp.maximum(acc[h], 0.0)).astype(jnp.bfloat16)

    def project(j, _):
        q = quad_of(j)

        @pl.when(lax.rem(j, 2) == 0)
        def _():
            from_sibling(q, down, down_sib)

        total = None
        for h in range(2):
            weights = down[pl.ds(4 * q, 4), h].reshape(quad, mine)
            term = lax.dot_general(
                hidden[h, chunk_rows(j), :], weights, (((1,), (1,)), ((), ())), preferred_element_type=jnp.float32
            )
            total = term if total is None else total + term
        part[j] = total.astype(jnp.bfloat16)

        @pl.when(jnp.logical_not(home))
        def _():
            remote(part.at[j], ypart.at[j], y_out, y_in.at[j], grp=partner).start()

        return 0

    norm_at = 7 + 5 * c

    def ring_pass(s, _):
        @pl.when(s <= last)
        def _():
            ring_step(s, *up_args)

        @pl.when(s == lag)
        def _():
            begin(*down_args)

        @pl.when(s > lag)
        def _():
            ring_step(s - lag, *down_args)

        @pl.when((s >= norm_at) & (s < norm_at + TOKEN_PARTS))
        def _():
            normalize(s - norm_at)

        over = s - last

        @pl.when(near & (over >= -1) & (over < 3))
        def _():
            lax.fori_loop(2 * over + 2, 2 * over + 4, lift, 0)

        @pl.when(near & (over == 2))
        def _():
            activate()

        @pl.when(near & (over >= 3))
        def _():
            lax.fori_loop(2 * over - 6, 2 * over - 4, project, 0)

        return 0

    lax.fori_loop(1, last + lag + 1, ring_pass, 0)

    @pl.when(jnp.logical_not(near))
    def _():
        lax.fori_loop(0, n_quads, lift, 0)
        activate()

    made = jnp.where(near, 2 * (lag - 2), 0)

    def pair_sum(j):
        arrived(ypart.at[j], y_in.at[j])
        part[j] = (part[j].astype(jnp.float32) + ypart[j].astype(jnp.float32)).astype(jnp.bfloat16)
        for i in range(1, nx):
            view = pl.ds(pl.multiple_of(peer(i) * own, own), own)
            slot = nx - 1 - i
            remote(
                part.at[j, view], xpart.at[slot, j], x_out, x_in.at[slot * n_chunks + j], tp=2 * peer(i) + c
            ).start()

    def row_sum(j):
        q = quad_of(j)
        total = part[j, pl.ds(pl.multiple_of(x * own, own), own), :].astype(jnp.float32)
        for i in range(nx - 1):
            arrived(xpart.at[i, j], x_in.at[i * n_chunks + j])
            total += xpart[i, j].astype(jnp.float32)
        branch[q, chunk_rows(j, x), :] = total.astype(jnp.bfloat16)
        view = branch.at[q, chunk_rows(j, x)]
        for i in (1, nx - 1):
            remote(view, view, all_out, all_in.at[(nx - 1 - i) * n_chunks + j], tp=2 * peer(i) + c).start()
        remote(view, view, all_sib_out, branch_sib.at[j], tp=sibling).start()

    def take(i, j):
        view = branch.at[quad_of(j), chunk_rows(j, peer(i))]
        arrived(view, all_in.at[(i - 1) * n_chunks + j])
        remote(view, view, all_sib_out, branch_sib.at[j], tp=sibling).start()
        return view

    def hand_on(j):
        view = take(1, j)
        remote(view, view, all_out, all_in.at[n_chunks + j], tp=2 * peer(nx - 1) + c).start()
        take(nx - 1, j)

    def write(j):
        view = (quad_of(j), chunk_rows(j))
        pltpu.make_async_copy(branch.at[view], out.at[view], out_sem.at[j]).start()

    def hand_far(j):
        take(2, j)
        write(j)

    stages = ((1, pair_sum), (4, row_sum), (7, hand_on), (10, hand_far))

    def output_pass(i, _):
        @pl.when(made + i < n_chunks)
        def _():
            project(made + i, 0)

        @pl.when(home)
        def _():
            for behind, stage in stages:

                @pl.when((i >= behind) & (i < n_chunks + behind))
                def _():
                    stage(i - behind)

        return 0

    lax.fori_loop(0, n_chunks + stages[-1][0], output_pass, 0)

    for side in range(2):

        @pl.when(c == side)
        def _():
            for sem in (up_out, down_out, up_sib_out, down_sib_out):
                arrived(up.at[pl.ds(0, reach[side])], sem)

    arrived(up.at[0], own_sib_out)

    @pl.when(home)
    def _():
        arrived(seen, tok_out)
        most = part.at[pl.ds(0, n_chunks * (nx - 1) // nx)]
        arrived(most, x_out)
        arrived(most, all_out)
        arrived(part, all_sib_out)

    @pl.when(jnp.logical_not(home))
    def _():
        arrived(part, y_out)

        def write_arrived(j, _):
            arrived(part.at[j], branch_sib.at[j])
            write(j)
            return 0

        lax.fori_loop(0, n_chunks, write_arrived, 0)

    def written(j, _):
        arrived(part.at[j], out_sem.at[j])
        return 0

    lax.fori_loop(0, n_chunks, written, 0)


def finish(branch, tok, post, out):
    n_quads, _, quad = branch.shape
    values = branch[...].astype(jnp.float32)
    squares = jnp.sum(jnp.sum(values * values, axis=0), axis=-1, keepdims=True)
    scale = lax.rsqrt(squares / (n_quads * quad) + epsilon)
    for q in range(n_quads):
        cols = slice(q * quad, (q + 1) * quad)
        result = tok[:, cols].astype(jnp.float32) + values[q] * scale * post[:, cols]
        out[:, cols] = result.astype(jnp.bfloat16)


def solution(mesh):
    nz, nx = mesh.shape["fs"], mesh.shape["tp"] // 2

    def on_device(tokens, pre_gain, up_weight, up_scale, down_weight, down_scale, post_gain):
        rows, width = tokens.shape
        block, units = up_weight.shape
        mine = units // 2
        quad = 4 * block
        n_quads = width // quad
        n_chunks = 2 * n_quads
        tall = rows // 2
        own = tall // nx
        vmem = pl.BlockSpec(memory_space=pltpu.VMEM)
        bf16, f32 = jnp.bfloat16, jnp.float32
        dma = pltpu.SemaphoreType.DMA
        anywhere = pl.BlockSpec(memory_space=pl.ANY)
        branch = pl.pallas_call(
            functools.partial(kernel, nz, nx),
            out_shape=jax.ShapeDtypeStruct((n_quads, rows, quad), bf16),
            in_specs=[anywhere] + [vmem] * 5,
            out_specs=anywhere,
            scratch_shapes=[
                pltpu.VMEM((nz, 2, block, mine), bf16),
                pltpu.VMEM((nz, 2, block, mine), bf16),
                pltpu.VMEM((rows, width), bf16),
                pltpu.VMEM((n_quads, rows, quad), bf16),
                pltpu.VMEM((2, rows, mine), f32),
                pltpu.VMEM((2, rows, mine), bf16),
                pltpu.VMEM((n_chunks, tall, quad), bf16),
                pltpu.VMEM((n_chunks, tall, quad), bf16),
                pltpu.VMEM((nx - 1, n_chunks, own, quad), bf16),
                pltpu.VMEM((n_quads, rows, quad), bf16),
                dma((nz * 2 * PARTS,)),
                dma((nz * 2 * PARTS,)),
                dma((nz,)),
                dma((nz,)),
                dma((TOKEN_PARTS,)),
                dma((n_chunks,)),
                dma(((nx - 1) * n_chunks,)),
                dma(((nx - 1) * n_chunks,)),
                dma((n_chunks,)),
                dma,
                dma,
                dma,
                dma,
                dma,
                dma,
                dma,
                dma,
                dma,
                dma,
                dma((n_chunks,)),
            ],
            compiler_params=pltpu.CompilerParams(
                collective_id=0, has_side_effects=True, vmem_limit_bytes=60 * 1024 * 1024
            ),
        )(
            tokens,
            pre_gain.reshape(1, width),
            up_weight,
            up_scale.reshape(1, units),
            down_weight.T,
            down_scale.reshape(1, block),
        )
        step = rows // 8
        return pl.pallas_call(
            finish,
            grid=(rows // step,),
            out_shape=jax.ShapeDtypeStruct((rows, width), bf16),
            in_specs=[
                pl.BlockSpec((n_quads, step, quad), lambda i: (0, i, 0)),
                pl.BlockSpec((step, width), lambda i: (i, 0)),
                pl.BlockSpec((1, width), lambda i: (0, 0)),
            ],
            out_specs=pl.BlockSpec((step, width), lambda i: (i, 0)),
        )(branch, tokens, post_gain.reshape(1, width))

    placed = (P(("grp", "fs"), None), P(), P("fs", "tp"), P("tp"), P("tp", "fs"), P("fs"), P())
    return jax.shard_map(
        on_device, mesh=mesh, in_specs=placed, out_specs=P(("grp", "fs"), None), check_vma=False
    )
```

```python
import functools

import jax
import jax.numpy as jnp
from jax import lax
from jax.experimental import pallas as pl
from jax.experimental.pallas import tpu as pltpu
from jax.sharding import PartitionSpec as P

epsilon = 1e-06
MESH = pl.DeviceIdType.MESH

LAG = (8, 4)
UP_PARTS, DOWN_PARTS = 4, 2
TICKS = (5, 3)
TOKEN_PARTS = 4
LIFTS = ((1, 8, 2, 7, 6, 5, 3, 4), (1, 8, 2, 7, 3, 6, 5, 4))
ORDER = (1, 2, 0, 3, 7, 4, 6, 5)


def remote(src, dst, send_sem, recv_sem, **where):
    return pltpu.make_async_remote_copy(
        src_ref=src, dst_ref=dst, send_sem=send_sem, recv_sem=recv_sem, device_id=where, device_id_type=MESH
    )


def arrived(ref, sem):
    pltpu.make_async_copy(ref, ref, sem).wait()


def reaches(nz):
    return nz * 12 // 32, nz - 1 - nz * 12 // 32


def kernel(
    nz, nx, tok, gain, up_w, up_s, down_w, down_s, out,
    up, down, seen, normed, acc, hidden, part, ypart, xpart, branch,
    up_in, down_in, up_sib, down_sib, own_sib, tok_in, y_in, x_in, all_in, branch_sib,
    up_out, down_out, up_sib_out, down_sib_out, own_sib_out, tok_out, y_out, x_out, all_out, all_sib_out, out_sem,
):
    rows, width = tok.shape
    block, units = up_w.shape
    mine = units // 2
    quad = 4 * block
    n_quads = width // quad
    n_chunks = 2 * n_quads
    tall = rows // 2
    own = tall // nx
    tok_rows = rows // TOKEN_PARTS
    reach = reaches(nz)

    g = lax.axis_index("grp")
    z = lax.axis_index("fs")
    t = lax.axis_index("tp")
    y = lax.rem(g, 2)
    c = lax.rem(t, 2)
    x = t // 2
    partner = g + 1 - 2 * y
    sibling = t + 1 - 2 * c
    way = 1 - 2 * c
    following = lax.rem(z + way + nz, nz)
    previous = lax.rem(z - way + nz, nz)
    home = c == y
    z_quad = z // 4
    last = jnp.where(c == 0, reach[0], reach[1])
    lag = jnp.where(c == 0, LAG[0], LAG[1])
    near = z < nz // 2

    def peer(i):
        return lax.rem(x + i, nx)

    barrier = pltpu.get_barrier_semaphore()
    neighbours = [{"fs": previous}, {"tp": sibling}, {"grp": partner}]
    neighbours += [{"tp": 2 * peer(i) + c} for i in range(1, nx)]
    for where in neighbours:
        pl.semaphore_signal(barrier, inc=1, device_id=where, device_id_type=MESH)

    def token_rows(k):
        return pl.ds(pl.multiple_of(k * tok_rows, tok_rows), tok_rows)

    @pl.when(home)
    def _():
        for k in range(TOKEN_PARTS):
            pltpu.make_async_copy(tok.at[token_rows(k)], seen.at[token_rows(k)], tok_in.at[k]).start()

    half = pl.ds(pl.multiple_of(y * mine, mine), mine)
    up[z, c] = (up_w[:, half] * up_s[:, half]).astype(jnp.bfloat16)
    line = lax.broadcasted_iota(jnp.int32, (block, block), 0) == lax.broadcasted_iota(jnp.int32, (block, block), 1)
    column = jnp.sum(jnp.where(line, jnp.broadcast_to(down_s[...], (block, block)), 0.0), axis=1, keepdims=True)
    down[z, c] = (down_w[:, half] * column).astype(jnp.bfloat16)
    pl.semaphore_wait(barrier, len(neighbours))

    def pick(values, i):
        return sum(jnp.where(i == k, v, 0) for k, v in enumerate(values))

    def quad_of(j):
        return lax.rem(z_quad + pick(ORDER, j // 2), n_quads)

    def chunk_rows(j, of=None):
        first = lax.rem(j, 2) * tall
        if of is None:
            return pl.ds(pl.multiple_of(first, tall), tall)
        return pl.ds(pl.multiple_of(first + of * own, own), own)

    def send_half(s, b, h, buf, in_sem, out_sem, parts):
        piece = block // parts
        for k in range(parts):
            view = buf.at[b, h, pl.ds(k * piece, piece)]

            def slot(step):
                return in_sem.at[(2 * (step - 1) + h) * parts + k]

            if s is None:
                remote(view, view, out_sem, slot(1), fs=following).start()
                continue
            arrived(view, slot(s))

            @pl.when(s < last)
            def _():
                remote(view, view, out_sem, slot(s + 1), fs=following).start()

    def begin(buf, in_sem, sib_sem, out_sem, sib_out, own_sem, parts):
        send_half(None, z, c, buf, in_sem, out_sem, parts)
        arrived(buf.at[z, 1 - c], own_sem)
        send_half(None, z, 1 - c, buf, in_sem, out_sem, parts)

    def ring_step(s, buf, in_sem, sib_sem, out_sem, sib_out, own_sem, parts):
        b = lax.rem(z - way * s + nz, nz)
        for h in (c, 1 - c):
            send_half(s, b, h, buf, in_sem, out_sem, parts)
        remote(buf.at[b], buf.at[b], sib_out, sib_sem.at[b // 4], tp=sibling).start()

    def from_sibling(q, buf, sib_sem):
        count = 0
        for i in range(4):
            ahead = lax.rem(4 * q + i - z + nz, nz)
            theirs = (ahead > 0) & jnp.where(c == 0, ahead <= reach[1], ahead > reach[1])
            count += jnp.where(theirs, 1, 0)
        for n in range(1, 5):

            @pl.when(count == n)
            def _():
                arrived(buf.at[pl.ds(0, n)], sib_sem.at[q])

    up_args = (up, up_in, up_sib, up_out, up_sib_out, own_sib.at[0], UP_PARTS)
    down_args = (down, down_in, down_sib, down_out, down_sib_out, own_sib.at[1], DOWN_PARTS)
    for k, buf in enumerate((up, down)):
        remote(buf.at[z, c], buf.at[z, c], own_sib_out, own_sib.at[k], tp=sibling).start()

    @pl.when(home)
    def _():
        for k in range(TOKEN_PARTS):
            remote(tok.at[token_rows(k)], seen.at[token_rows(k)], tok_out, tok_in.at[k], grp=partner).start()

    begin(*up_args)
    acc[...] = jnp.zeros_like(acc)

    def normalize(k):
        arrived(seen.at[token_rows(k)], tok_in.at[k])
        step = 32

        def body(i, _):
            view = pl.ds(pl.multiple_of(k * tok_rows + i * step, step), step)
            values = seen[view, :].astype(jnp.float32)
            mean = jnp.mean(values * values, axis=-1, keepdims=True)
            scaled = (values * lax.rsqrt(mean + epsilon) * gain[...]).astype(jnp.bfloat16)
            for q in range(n_quads):
                normed[q, view, :] = scaled[:, q * quad : (q + 1) * quad]
            return 0

        lax.fori_loop(0, tok_rows // step, body, 0)

    def lift(i, _):
        m = jnp.where(c == 0, pick(LIFTS[0], i), pick(LIFTS[1], i))
        q = lax.rem(z_quad - way * m + n_quads + 8, n_quads)
        from_sibling(q, up, up_sib)
        for h in range(2):
            weights = up[pl.ds(4 * q, 4), h].reshape(quad, mine)
            acc[h] += jnp.dot(normed[q], weights, preferred_element_type=jnp.float32)
        return 0

    def activate():
        for h in range(2):
            hidden[h] = jnp.square(jnp.maximum(acc[h], 0.0)).astype(jnp.bfloat16)

    def project(j, _):
        q = quad_of(j)

        @pl.when(lax.rem(j, 2) == 0)
        def _():
            from_sibling(q, down, down_sib)

        total = None
        for h in range(2):
            weights = down[pl.ds(4 * q, 4), h].reshape(quad, mine)
            term = lax.dot_general(
                hidden[h, chunk_rows(j), :], weights, (((1,), (1,)), ((), ())), preferred_element_type=jnp.float32
            )
            total = term if total is None else total + term
        part[j] = total.astype(jnp.bfloat16)

        @pl.when(jnp.logical_not(home))
        def _():
            remote(part.at[j], ypart.at[j], y_out, y_in.at[j], grp=partner).start()

        return 0

    def pair_sum(j):
        arrived(ypart.at[j], y_in.at[j])
        part[j] = (part[j].astype(jnp.float32) + ypart[j].astype(jnp.float32)).astype(jnp.bfloat16)
        for i in range(1, nx):
            view = pl.ds(pl.multiple_of(peer(i) * own, own), own)
            slot = nx - 1 - i
            remote(
                part.at[j, view], xpart.at[j, slot], x_out, x_in.at[j], tp=2 * peer(i) + c
            ).start()

    def row_sum(j):
        q = quad_of(j)
        total = part[j, pl.ds(pl.multiple_of(x * own, own), own), :].astype(jnp.float32)
        arrived(xpart.at[j], x_in.at[j])
        for i in range(nx - 1):
            total += xpart[j, i].astype(jnp.float32)
        branch[q, chunk_rows(j, x), :] = total.astype(jnp.bfloat16)
        view = branch.at[q, chunk_rows(j, x)]
        for i in (1, nx - 1):
            remote(view, view, all_out, all_in.at[j], tp=2 * peer(i) + c).start()
        remote(view, view, all_sib_out, branch_sib.at[j], tp=sibling).start()

    def pass_on(i, j):
        view = branch.at[quad_of(j), chunk_rows(j, peer(i))]
        remote(view, view, all_sib_out, branch_sib.at[j], tp=sibling).start()
        return view

    def hand_on(j):
        arrived(part.at[j, pl.ds(0, 2 * own)], all_in.at[j])
        view = pass_on(1, j)
        remote(view, view, all_out, all_in.at[n_chunks + j], tp=2 * peer(nx - 1) + c).start()
        pass_on(nx - 1, j)

    def write(j):
        view = (quad_of(j), chunk_rows(j))
        pltpu.make_async_copy(branch.at[view], out.at[view], out_sem).start()

    def hand_far(j):
        arrived(part.at[j, pl.ds(0, own)], all_in.at[n_chunks + j])
        pass_on(2, j)
        write(j)

    stages = ((1, pair_sum), (4, row_sum), (7, hand_on), (10, hand_far))

    def tick(i, _):
        for behind, stage in stages:

            @pl.when((i >= behind) & (i < n_chunks + behind))
            def _():
                stage(i - behind)

        return 0

    ready = jnp.where(c == 0, 2, 0)
    ticks_at = jnp.where(c == 0, TICKS[0], TICKS[1])

    def lifts_at(over):
        return jnp.clip(2 * over + 2, 0, n_quads) * (1 - c) + jnp.where(
            over > 0, n_quads, jnp.clip(2 * over + 4, 0, n_quads)
        ) * c

    norm_at = 7 + 5 * c

    def ring_pass(s, _):
        @pl.when(s <= last)
        def _():
            ring_step(s, *up_args)

        @pl.when(s == lag)
        def _():
            begin(*down_args)

        @pl.when(s > lag)
        def _():
            ring_step(s - lag, *down_args)

        @pl.when((s >= norm_at) & (s < norm_at + TOKEN_PARTS))
        def _():
            normalize(s - norm_at)

        over = s - last

        lo, hi = lifts_at(over), lifts_at(over + 1)

        @pl.when(near & (hi > lo))
        def _():
            lax.fori_loop(lo, hi, lift, 0)

        @pl.when(near & (over == ready))
        def _():
            activate()

        @pl.when(near & (over > ready))
        def _():
            lax.fori_loop(2 * (over - ready) - 2, 2 * (over - ready), project, 0)

        @pl.when(near & home & (over >= ticks_at))
        def _():
            lax.fori_loop(2 * (over - ticks_at) + 1, 2 * (over - ticks_at) + 3, tick, 0)

        return 0

    lax.fori_loop(1, last + lag + 1, ring_pass, 0)

    @pl.when(jnp.logical_not(near))
    def _():
        lax.fori_loop(0, n_quads, lift, 0)
        activate()

    made = jnp.where(near, 2 * (lag - ready), 0)
    ticked = jnp.where(near, 2 * (lag - ticks_at + 1) + 1, 0)

    def output_pass(i, _):
        @pl.when(made + i < n_chunks)
        def _():
            project(made + i, 0)

        @pl.when(home)
        def _():
            tick(ticked + i, 0)

        return 0

    lax.fori_loop(0, n_chunks + stages[-1][0], output_pass, 0)

    for side in range(2):

        @pl.when(c == side)
        def _():
            for sem in (up_out, down_out, up_sib_out, down_sib_out):
                arrived(up.at[pl.ds(0, reach[side])], sem)

    arrived(up.at[0], own_sib_out)

    @pl.when(home)
    def _():
        arrived(seen, tok_out)
        most = part.at[pl.ds(0, n_chunks * (nx - 1) // nx)]
        arrived(most, x_out)
        arrived(most, all_out)
        arrived(part, all_sib_out)

    @pl.when(jnp.logical_not(home))
    def _():
        arrived(part, y_out)

        def write_arrived(j, _):
            arrived(part.at[j], branch_sib.at[j])
            write(j)
            return 0

        lax.fori_loop(0, n_chunks, write_arrived, 0)

    arrived(part, out_sem)


def finish(branch, tok, post, out):
    n_quads, _, quad = branch.shape
    values = branch[...].astype(jnp.float32)
    squares = jnp.sum(jnp.sum(values * values, axis=0), axis=-1, keepdims=True)
    scale = lax.rsqrt(squares / (n_quads * quad) + epsilon)
    for q in range(n_quads):
        cols = slice(q * quad, (q + 1) * quad)
        result = tok[:, cols].astype(jnp.float32) + values[q] * scale * post[:, cols]
        out[:, cols] = result.astype(jnp.bfloat16)


def solution(mesh):
    nz, nx = mesh.shape["fs"], mesh.shape["tp"] // 2

    def on_device(tokens, pre_gain, up_weight, up_scale, down_weight, down_scale, post_gain):
        rows, width = tokens.shape
        block, units = up_weight.shape
        mine = units // 2
        quad = 4 * block
        n_quads = width // quad
        n_chunks = 2 * n_quads
        tall = rows // 2
        own = tall // nx
        longest = max(reaches(nz))
        vmem = pl.BlockSpec(memory_space=pltpu.VMEM)
        bf16, f32 = jnp.bfloat16, jnp.float32
        dma = pltpu.SemaphoreType.DMA
        anywhere = pl.BlockSpec(memory_space=pl.ANY)
        branch = pl.pallas_call(
            functools.partial(kernel, nz, nx),
            out_shape=jax.ShapeDtypeStruct((n_quads, rows, quad), bf16),
            in_specs=[anywhere] + [vmem] * 5,
            out_specs=anywhere,
            scratch_shapes=[
                pltpu.VMEM((nz, 2, block, mine), bf16),
                pltpu.VMEM((nz, 2, block, mine), bf16),
                pltpu.VMEM((rows, width), bf16),
                pltpu.VMEM((n_quads, rows, quad), bf16),
                pltpu.VMEM((2, rows, mine), f32),
                pltpu.VMEM((2, rows, mine), bf16),
                pltpu.VMEM((n_chunks, tall, quad), bf16),
                pltpu.VMEM((n_chunks, tall, quad), bf16),
                pltpu.VMEM((n_chunks, nx - 1, own, quad), bf16),
                pltpu.VMEM((n_quads, rows, quad), bf16),
                dma((longest * 2 * UP_PARTS,)),
                dma((longest * 2 * DOWN_PARTS,)),
                dma((n_quads,)),
                dma((n_quads,)),
                dma((2,)),
                dma((TOKEN_PARTS,)),
                dma((n_chunks,)),
                dma((n_chunks,)),
                dma((2 * n_chunks,)),
                dma((n_chunks,)),
                dma,
                dma,
                dma,
                dma,
                dma,
                dma,
                dma,
                dma,
                dma,
                dma,
                dma,
            ],
            compiler_params=pltpu.CompilerParams(
                collective_id=0, has_side_effects=True, vmem_limit_bytes=60 * 1024 * 1024
            ),
        )(
            tokens,
            pre_gain.reshape(1, width),
            up_weight,
            up_scale.reshape(1, units),
            down_weight.T,
            down_scale.reshape(1, block),
        )
        step = rows // 8
        return pl.pallas_call(
            finish,
            grid=(rows // step,),
            out_shape=jax.ShapeDtypeStruct((rows, width), bf16),
            in_specs=[
                pl.BlockSpec((n_quads, step, quad), lambda i: (0, i, 0)),
                pl.BlockSpec((step, width), lambda i: (i, 0)),
                pl.BlockSpec((1, width), lambda i: (0, 0)),
            ],
            out_specs=pl.BlockSpec((step, width), lambda i: (i, 0)),
        )(branch, tokens, post_gain.reshape(1, width))

    placed = (P(("grp", "fs"), None), P(), P("fs", "tp"), P("tp"), P("tp", "fs"), P("fs"), P())
    return jax.shard_map(
        on_device, mesh=mesh, in_specs=placed, out_specs=P(("grp", "fs"), None), check_vma=False
    )
```

```python
import functools

import jax
import jax.numpy as jnp
from jax import lax
from jax.experimental import pallas as pl
from jax.experimental.pallas import tpu as pltpu
from jax.sharding import PartitionSpec as P

epsilon = 1e-06
MESH = pl.DeviceIdType.MESH

LAG = (8, 6)
UP_PARTS, DOWN_PARTS = 4, 2
TICKS = (5, 3)
TOKEN_PARTS = 4
LIFTS = ((1, 8, 2, 7, 6, 5, 3, 4), (1, 8, 2, 7, 3, 6, 5, 4))
ORDER = (1, 2, 0, 3, 7, 6, 4, 5)


def remote(src, dst, send_sem, recv_sem, **where):
    return pltpu.make_async_remote_copy(
        src_ref=src, dst_ref=dst, send_sem=send_sem, recv_sem=recv_sem, device_id=where, device_id_type=MESH
    )


def arrived(ref, sem):
    pltpu.make_async_copy(ref, ref, sem).wait()


def reaches(nz):
    return nz * 13 // 32, nz - 1 - nz * 13 // 32


def kernel(
    nz, nx, tok, gain_in, up_w_in, up_s_in, down_w_in, down_s_in, out, scale_out,
    gain, up_w, up_s, down_w, down_s, squares, up, down, seen, normed, acc, hidden, part, ypart, xpart, branch,
    up_in, down_in, up_sib, down_sib, own_sib, tok_in, y_in, x_in, all_in, branch_sib,
    up_out, down_out, up_sib_out, down_sib_out, own_sib_out, tok_out, y_out, x_out, all_out, all_sib_out, out_sem, fetched, scale_sem,
):
    rows, width = tok.shape
    block, units = up_w_in.shape
    mine = units // 2
    quad = 4 * block
    n_quads = width // quad
    n_chunks = 2 * n_quads
    tall = rows // 2
    own = tall // nx
    tok_rows = rows // TOKEN_PARTS
    reach = reaches(nz)

    g = lax.axis_index("grp")
    z = lax.axis_index("fs")
    t = lax.axis_index("tp")
    y = lax.rem(g, 2)
    c = lax.rem(t, 2)
    x = t // 2
    partner = g + 1 - 2 * y
    sibling = t + 1 - 2 * c
    way = 1 - 2 * c
    following = lax.rem(z + way + nz, nz)
    previous = lax.rem(z - way + nz, nz)
    home = c == y
    z_quad = z // 4
    last = jnp.where(c == 0, reach[0], reach[1])
    lag = jnp.where(c == 0, LAG[0], LAG[1])
    near = z < nz // 2

    def peer(i):
        return lax.rem(x + i, nx)

    fetches = [
        pltpu.make_async_copy(src, dst, fetched.at[k])
        for k, (src, dst) in enumerate(
            ((up_w_in, up_w), (up_s_in, up_s), (down_w_in, down_w), (down_s_in, down_s), (gain_in, gain))
        )
    ]
    for fetch in fetches:
        fetch.start()
    barrier = pltpu.get_barrier_semaphore()
    neighbours = [{"fs": previous}, {"tp": sibling}, {"grp": partner}]
    neighbours += [{"tp": 2 * peer(i) + c} for i in range(1, nx)]
    for where in neighbours:
        pl.semaphore_signal(barrier, inc=1, device_id=where, device_id_type=MESH)

    def token_rows(k):
        return pl.ds(pl.multiple_of(k * tok_rows, tok_rows), tok_rows)

    @pl.when(home)
    def _():
        for k in range(TOKEN_PARTS):
            pltpu.make_async_copy(tok.at[token_rows(k)], seen.at[token_rows(k)], tok_in.at[k]).start()

    for fetch in fetches:
        fetch.wait()
    half = pl.ds(pl.multiple_of(y * mine, mine), mine)
    up[z, c] = (up_w[:, half] * up_s[:, half]).astype(jnp.bfloat16)
    line = lax.broadcasted_iota(jnp.int32, (block, block), 0) == lax.broadcasted_iota(jnp.int32, (block, block), 1)
    column = jnp.sum(jnp.where(line, jnp.broadcast_to(down_s[...], (block, block)), 0.0), axis=1, keepdims=True)
    down[z, c] = (down_w[:, half] * column).astype(jnp.bfloat16)
    pl.semaphore_wait(barrier, len(neighbours))

    def pick(values, i):
        return sum(jnp.where(i == k, v, 0) for k, v in enumerate(values))

    def quad_of(j):
        return lax.rem(z_quad + pick(ORDER, j // 2), n_quads)

    def chunk_rows(j, of=None):
        first = lax.rem(j, 2) * tall
        if of is None:
            return pl.ds(pl.multiple_of(first, tall), tall)
        return pl.ds(pl.multiple_of(first + of * own, own), own)

    def send_half(s, b, h, buf, in_sem, out_sem, parts):
        piece = block // parts
        for k in range(parts):
            view = buf.at[b, h, pl.ds(k * piece, piece)]

            def slot(step):
                return in_sem.at[(2 * (step - 1) + h) * parts + k]

            if s is None:
                remote(view, view, out_sem, slot(1), fs=following).start()
                continue
            arrived(view, slot(s))

            @pl.when(s < last)
            def _():
                remote(view, view, out_sem, slot(s + 1), fs=following).start()

    def begin(buf, in_sem, sib_sem, out_sem, sib_out, own_sem, parts):
        send_half(None, z, c, buf, in_sem, out_sem, parts)
        arrived(buf.at[z, 1 - c], own_sem)
        send_half(None, z, 1 - c, buf, in_sem, out_sem, parts)

    def ring_step(s, buf, in_sem, sib_sem, out_sem, sib_out, own_sem, parts):
        b = lax.rem(z - way * s + nz, nz)
        for h in (c, 1 - c):
            send_half(s, b, h, buf, in_sem, out_sem, parts)
        remote(buf.at[b], buf.at[b], sib_out, sib_sem.at[b // 4], tp=sibling).start()

    def from_sibling(q, buf, sib_sem):
        count = 0
        for i in range(4):
            ahead = lax.rem(4 * q + i - z + nz, nz)
            theirs = (ahead > 0) & jnp.where(c == 0, ahead <= reach[1], ahead > reach[1])
            count += jnp.where(theirs, 1, 0)
        for n in range(1, 5):

            @pl.when(count == n)
            def _():
                arrived(buf.at[pl.ds(0, n)], sib_sem.at[q])

    up_args = (up, up_in, up_sib, up_out, up_sib_out, own_sib.at[0], UP_PARTS)
    down_args = (down, down_in, down_sib, down_out, down_sib_out, own_sib.at[1], DOWN_PARTS)
    for k, buf in enumerate((up, down)):
        remote(buf.at[z, c], buf.at[z, c], own_sib_out, own_sib.at[k], tp=sibling).start()

    @pl.when(home)
    def _():
        for k in range(TOKEN_PARTS):
            remote(tok.at[token_rows(k)], seen.at[token_rows(k)], tok_out, tok_in.at[k], grp=partner).start()

    begin(*up_args)
    acc[...] = jnp.zeros_like(acc)
    squares[...] = jnp.zeros_like(squares)

    def normalize(k):
        arrived(seen.at[token_rows(k)], tok_in.at[k])
        step = 32

        def body(i, _):
            view = pl.ds(pl.multiple_of(k * tok_rows + i * step, step), step)
            values = seen[view, :].astype(jnp.float32)
            mean = jnp.mean(values * values, axis=-1, keepdims=True)
            scaled = (values * lax.rsqrt(mean + epsilon) * gain[...]).astype(jnp.bfloat16)
            for q in range(n_quads):
                normed[q, view, :] = scaled[:, q * quad : (q + 1) * quad]
            return 0

        lax.fori_loop(0, tok_rows // step, body, 0)

    def lift(i, _):
        m = jnp.where(c == 0, pick(LIFTS[0], i), pick(LIFTS[1], i))
        q = lax.rem(z_quad - way * m + n_quads + 8, n_quads)
        from_sibling(q, up, up_sib)
        for h in range(2):
            weights = up[pl.ds(4 * q, 4), h].reshape(quad, mine)
            acc[h] += jnp.dot(normed[q], weights, preferred_element_type=jnp.float32)
        return 0

    def activate():
        for h in range(2):
            hidden[h] = jnp.square(jnp.maximum(acc[h], 0.0)).astype(jnp.bfloat16)

    def project(j, _):
        q = quad_of(j)

        @pl.when(lax.rem(j, 2) == 0)
        def _():
            from_sibling(q, down, down_sib)

        total = None
        for h in range(2):
            weights = down[pl.ds(4 * q, 4), h].reshape(quad, mine)
            term = lax.dot_general(
                hidden[h, chunk_rows(j), :], weights, (((1,), (1,)), ((), ())), preferred_element_type=jnp.float32
            )
            total = term if total is None else total + term
        part[j] = total.astype(jnp.bfloat16)

        @pl.when(jnp.logical_not(home))
        def _():
            remote(part.at[j], ypart.at[j], y_out, y_in.at[j], grp=partner).start()

        return 0

    def pair_sum(j):
        arrived(ypart.at[j], y_in.at[j])
        part[j] = (part[j].astype(jnp.float32) + ypart[j].astype(jnp.float32)).astype(jnp.bfloat16)
        for i in range(1, nx):
            view = pl.ds(pl.multiple_of(peer(i) * own, own), own)
            slot = nx - 1 - i
            remote(
                part.at[j, view], xpart.at[j, slot], x_out, x_in.at[j], tp=2 * peer(i) + c
            ).start()

    def row_sum(j):
        q = quad_of(j)
        total = part[j, pl.ds(pl.multiple_of(x * own, own), own), :].astype(jnp.float32)
        arrived(xpart.at[j], x_in.at[j])
        for i in range(nx - 1):
            total += xpart[j, i].astype(jnp.float32)
        branch[q, chunk_rows(j, x), :] = total.astype(jnp.bfloat16)
        view = branch.at[q, chunk_rows(j, x)]
        for i in (1, nx - 1):
            remote(view, view, all_out, all_in.at[j], tp=2 * peer(i) + c).start()
        remote(view, view, all_sib_out, branch_sib.at[j], tp=sibling).start()

    def pass_on(i, j):
        view = branch.at[quad_of(j), chunk_rows(j, peer(i))]
        remote(view, view, all_sib_out, branch_sib.at[j], tp=sibling).start()
        return view

    def hand_on(j):
        arrived(part.at[j, pl.ds(0, 2 * own)], all_in.at[j])
        view = pass_on(1, j)
        remote(view, view, all_out, all_in.at[n_chunks + j], tp=2 * peer(nx - 1) + c).start()
        pass_on(nx - 1, j)

    def write(j):
        view = (quad_of(j), chunk_rows(j))
        pltpu.make_async_copy(branch.at[view], out.at[view], out_sem).start()
        values = branch[view[0], view[1], :].astype(jnp.float32)
        values *= values
        lanes = squares.shape[1]
        squares[view[1], :] += sum(values[:, k : k + lanes] for k in range(0, quad, lanes))

    def hand_far(j):
        arrived(part.at[j, pl.ds(0, own)], all_in.at[n_chunks + j])
        pass_on(2, j)
        write(j)

    stages = ((1, pair_sum), (4, row_sum), (7, hand_on), (10, hand_far))

    def tick(i, _):
        for behind, stage in stages:

            @pl.when((i >= behind) & (i < n_chunks + behind))
            def _():
                stage(i - behind)

        return 0

    ready = jnp.where(c == 0, 2, 0)
    ticks_at = jnp.where(c == 0, TICKS[0], TICKS[1])

    def lifts_at(over):
        return jnp.clip(2 * over + 2, 0, n_quads) * (1 - c) + jnp.where(
            over > 0, n_quads, jnp.clip(2 * over + 4, 0, n_quads)
        ) * c

    norm_at = 8 + 3 * c

    def ring_pass(s, _):
        @pl.when(s <= last)
        def _():
            ring_step(s, *up_args)

        @pl.when(s == lag)
        def _():
            begin(*down_args)

        @pl.when(s > lag)
        def _():
            ring_step(s - lag, *down_args)

        @pl.when((s >= norm_at) & (s < norm_at + TOKEN_PARTS))
        def _():
            normalize(s - norm_at)

        over = s - last

        lo, hi = lifts_at(over), lifts_at(over + 1)

        @pl.when(near & (hi > lo))
        def _():
            lax.fori_loop(lo, hi, lift, 0)

        @pl.when(near & (over == ready))
        def _():
            activate()

        @pl.when(near & (over > ready))
        def _():
            lax.fori_loop(2 * (over - ready) - 2, 2 * (over - ready), project, 0)

        @pl.when(near & home & (over >= ticks_at))
        def _():
            lax.fori_loop(2 * (over - ticks_at) + 1, 2 * (over - ticks_at) + 3, tick, 0)

        return 0

    lax.fori_loop(1, last + lag + 1, ring_pass, 0)

    @pl.when(jnp.logical_not(near))
    def _():
        lax.fori_loop(0, n_quads, lift, 0)
        activate()

    made = jnp.where(near, 2 * (lag - ready), 0)
    ticked = jnp.where(near, 2 * (lag - ticks_at + 1) + 1, 0)

    def output_pass(i, _):
        @pl.when(made + i < n_chunks)
        def _():
            project(made + i, 0)

        @pl.when(home)
        def _():
            tick(ticked + i, 0)

        return 0

    lax.fori_loop(0, n_chunks + stages[-1][0], output_pass, 0)

    for side in range(2):

        @pl.when(c == side)
        def _():
            for sem in (up_out, down_out, up_sib_out, down_sib_out):
                arrived(up.at[pl.ds(0, reach[side])], sem)

    arrived(up.at[0], own_sib_out)

    @pl.when(home)
    def _():
        arrived(seen, tok_out)
        most = part.at[pl.ds(0, n_chunks * (nx - 1) // nx)]
        arrived(most, x_out)
        arrived(most, all_out)
        arrived(part, all_sib_out)

    @pl.when(jnp.logical_not(home))
    def _():
        arrived(part, y_out)

        def write_arrived(j, _):
            arrived(part.at[j], branch_sib.at[j])
            write(j)
            return 0

        lax.fori_loop(0, n_chunks, write_arrived, 0)

    total = jnp.sum(squares[...], axis=-1, keepdims=True)
    squares[...] = jnp.broadcast_to(lax.rsqrt(total / width + epsilon), squares.shape)
    written = pltpu.make_async_copy(squares, scale_out, scale_sem)
    written.start()
    arrived(part, out_sem)
    written.wait()


def finish(branch, scale, tok, post, out):
    n_quads, _, quad = branch.shape
    lanes = scale.shape[1]
    for q in range(n_quads):
        for k in range(0, quad, lanes):
            cols = slice(q * quad + k, q * quad + k + lanes)
            values = branch[q, :, k : k + lanes].astype(jnp.float32) * scale[...] * post[:, cols]
            out[:, cols] = (tok[:, cols].astype(jnp.float32) + values).astype(jnp.bfloat16)


def solution(mesh):
    nz, nx = mesh.shape["fs"], mesh.shape["tp"] // 2

    def on_device(tokens, pre_gain, up_weight, up_scale, down_weight, down_scale, post_gain):
        rows, width = tokens.shape
        block, units = up_weight.shape
        mine = units // 2
        quad = 4 * block
        n_quads = width // quad
        n_chunks = 2 * n_quads
        tall = rows // 2
        own = tall // nx
        longest = max(reaches(nz))
        bf16, f32 = jnp.bfloat16, jnp.float32
        dma = pltpu.SemaphoreType.DMA
        anywhere = pl.BlockSpec(memory_space=pl.ANY)
        branch, scale = pl.pallas_call(
            functools.partial(kernel, nz, nx),
            out_shape=(
                jax.ShapeDtypeStruct((n_quads, rows, quad), bf16),
                jax.ShapeDtypeStruct((rows, 128), f32),
            ),
            in_specs=[anywhere] * 6,
            out_specs=(anywhere, anywhere),
            scratch_shapes=[
                pltpu.VMEM((1, width), f32),
                pltpu.VMEM((block, units), f32),
                pltpu.VMEM((1, units), f32),
                pltpu.VMEM((block, units), f32),
                pltpu.VMEM((1, block), f32),
                pltpu.VMEM((rows, 128), f32),
                pltpu.VMEM((nz, 2, block, mine), bf16),
                pltpu.VMEM((nz, 2, block, mine), bf16),
                pltpu.VMEM((rows, width), bf16),
                pltpu.VMEM((n_quads, rows, quad), bf16),
                pltpu.VMEM((2, rows, mine), f32),
                pltpu.VMEM((2, rows, mine), bf16),
                pltpu.VMEM((n_chunks, tall, quad), bf16),
                pltpu.VMEM((n_chunks, tall, quad), bf16),
                pltpu.VMEM((n_chunks, nx - 1, own, quad), bf16),
                pltpu.VMEM((n_quads, rows, quad), bf16),
                dma((longest * 2 * UP_PARTS,)),
                dma((longest * 2 * DOWN_PARTS,)),
                dma((n_quads,)),
                dma((n_quads,)),
                dma((2,)),
                dma((TOKEN_PARTS,)),
                dma((n_chunks,)),
                dma((n_chunks,)),
                dma((2 * n_chunks,)),
                dma((n_chunks,)),
                dma,
                dma,
                dma,
                dma,
                dma,
                dma,
                dma,
                dma,
                dma,
                dma,
                dma,
                dma((5,)),
                dma,
            ],
            compiler_params=pltpu.CompilerParams(
                collective_id=0, has_side_effects=True, vmem_limit_bytes=60 * 1024 * 1024
            ),
        )(
            tokens,
            pre_gain.reshape(1, width),
            up_weight,
            up_scale.reshape(1, units),
            down_weight.T,
            down_scale.reshape(1, block),
        )
        step = rows // 8
        return pl.pallas_call(
            finish,
            grid=(rows // step,),
            out_shape=jax.ShapeDtypeStruct((rows, width), bf16),
            in_specs=[
                pl.BlockSpec((n_quads, step, quad), lambda i: (0, i, 0)),
                pl.BlockSpec((step, 128), lambda i: (i, 0)),
                pl.BlockSpec((step, width), lambda i: (i, 0)),
                pl.BlockSpec((1, width), lambda i: (0, 0)),
            ],
            out_specs=pl.BlockSpec((step, width), lambda i: (i, 0)),
        )(branch, scale, tokens, post_gain.reshape(1, width))

    placed = (P(("grp", "fs"), None), P(), P("fs", "tp"), P("tp"), P("tp", "fs"), P("fs"), P())
    return jax.shard_map(
        on_device, mesh=mesh, in_specs=placed, out_specs=P(("grp", "fs"), None), check_vma=False
    )
```

```python
import functools

import jax
import jax.numpy as jnp
from jax import lax
from jax.experimental import pallas as pl
from jax.experimental.pallas import tpu as pltpu
from jax.sharding import PartitionSpec as P

epsilon = 1e-06
MESH = pl.DeviceIdType.MESH

LAG = (8, 6)
UP_PARTS, DOWN_PARTS = 4, 2
TICKS = (4, 2)
TOKEN_PARTS = 4
FINISH_PARTS = 4
LIFTS = ((1, 8, 2, 7, 6, 5, 3, 4), (1, 8, 2, 7, 3, 6, 5, 4))
ORDER = (1, 2, 0, 3, 7, 6, 4, 5)


def remote(src, dst, send_sem, recv_sem, **where):
    return pltpu.make_async_remote_copy(
        src_ref=src, dst_ref=dst, send_sem=send_sem, recv_sem=recv_sem, device_id=where, device_id_type=MESH
    )


def arrived(ref, sem):
    pltpu.make_async_copy(ref, ref, sem).wait()


def reaches(nz):
    return nz * 13 // 32, nz - 1 - nz * 13 // 32


def kernel(
    nz, nx, tok, gain_in, up_w_in, up_s_in, down_w_in, down_s_in, out, scale_out,
    gain, up_w, up_s, down_w, down_s, squares, up, down, seen, normed, acc, hidden, part, ypart, xpart, branch,
    up_in, down_in, up_sib, down_sib, own_sib, tok_in, y_in, x_in, all_in, branch_sib,
    up_out, down_out, up_sib_out, down_sib_out, own_sib_out, tok_out, y_out, x_out, all_out, all_sib_out, out_sem, fetched, scale_sem,
):
    rows, width = tok.shape
    block, units = up_w_in.shape
    mine = units // 2
    quad = 4 * block
    n_quads = width // quad
    n_chunks = 2 * n_quads
    tall = rows // 2
    own = tall // nx
    tok_rows = rows // TOKEN_PARTS
    reach = reaches(nz)

    g = lax.axis_index("grp")
    z = lax.axis_index("fs")
    t = lax.axis_index("tp")
    y = lax.rem(g, 2)
    c = lax.rem(t, 2)
    x = t // 2
    partner = g + 1 - 2 * y
    sibling = t + 1 - 2 * c
    way = 1 - 2 * c
    following = lax.rem(z + way + nz, nz)
    previous = lax.rem(z - way + nz, nz)
    home = c == y
    z_quad = z // 4
    last = jnp.where(c == 0, reach[0], reach[1])
    lag = jnp.where(c == 0, LAG[0], LAG[1])
    near = (z < nz // 2) | (c == 1)

    def peer(i):
        return lax.rem(x + i, nx)

    fetches = [
        pltpu.make_async_copy(src, dst, fetched.at[k])
        for k, (src, dst) in enumerate(
            ((up_w_in, up_w), (up_s_in, up_s), (down_w_in, down_w), (down_s_in, down_s), (gain_in, gain))
        )
    ]
    for fetch in fetches:
        fetch.start()
    barrier = pltpu.get_barrier_semaphore()
    neighbours = [{"fs": previous}, {"tp": sibling}, {"grp": partner}]
    neighbours += [{"tp": 2 * peer(i) + c} for i in range(1, nx)]
    for where in neighbours:
        pl.semaphore_signal(barrier, inc=1, device_id=where, device_id_type=MESH)

    def token_rows(k):
        return pl.ds(pl.multiple_of(k * tok_rows, tok_rows), tok_rows)

    @pl.when(home)
    def _():
        for k in range(TOKEN_PARTS):
            pltpu.make_async_copy(tok.at[token_rows(k)], seen.at[token_rows(k)], tok_in.at[k]).start()

    for fetch in fetches:
        fetch.wait()
    half = pl.ds(pl.multiple_of(y * mine, mine), mine)
    up[z, c] = (up_w[:, half] * up_s[:, half]).astype(jnp.bfloat16)
    line = lax.broadcasted_iota(jnp.int32, (block, block), 0) == lax.broadcasted_iota(jnp.int32, (block, block), 1)
    column = jnp.sum(jnp.where(line, jnp.broadcast_to(down_s[...], (block, block)), 0.0), axis=1, keepdims=True)
    down[z, c] = (down_w[:, half] * column).astype(jnp.bfloat16)
    pl.semaphore_wait(barrier, len(neighbours))

    def pick(values, i):
        return sum(jnp.where(i == k, v, 0) for k, v in enumerate(values))

    def quad_of(j):
        return lax.rem(z_quad + pick(ORDER, j // 2), n_quads)

    def chunk_rows(j, of=None):
        first = lax.rem(j, 2) * tall
        if of is None:
            return pl.ds(pl.multiple_of(first, tall), tall)
        return pl.ds(pl.multiple_of(first + of * own, own), own)

    def send_half(s, b, h, buf, in_sem, out_sem, parts):
        piece = block // parts
        for k in range(parts):
            view = buf.at[b, h, pl.ds(k * piece, piece)]

            def slot(step):
                return in_sem.at[(2 * (step - 1) + h) * parts + k]

            if s is None:
                remote(view, view, out_sem, slot(1), fs=following).start()
                continue
            arrived(view, slot(s))

            @pl.when(s < last)
            def _():
                remote(view, view, out_sem, slot(s + 1), fs=following).start()

    def begin(buf, in_sem, sib_sem, out_sem, sib_out, own_sem, parts):
        send_half(None, z, c, buf, in_sem, out_sem, parts)
        arrived(buf.at[z, 1 - c], own_sem)
        send_half(None, z, 1 - c, buf, in_sem, out_sem, parts)

    def ring_step(s, buf, in_sem, sib_sem, out_sem, sib_out, own_sem, parts):
        b = lax.rem(z - way * s + nz, nz)
        for h in (c, 1 - c):
            send_half(s, b, h, buf, in_sem, out_sem, parts)
        remote(buf.at[b], buf.at[b], sib_out, sib_sem.at[b // 4], tp=sibling).start()

    def from_sibling(q, buf, sib_sem):
        count = 0
        for i in range(4):
            ahead = lax.rem(4 * q + i - z + nz, nz)
            theirs = (ahead > 0) & jnp.where(c == 0, ahead <= reach[1], ahead > reach[1])
            count += jnp.where(theirs, 1, 0)
        for n in range(1, 5):

            @pl.when(count == n)
            def _():
                arrived(buf.at[pl.ds(0, n)], sib_sem.at[q])

    up_args = (up, up_in, up_sib, up_out, up_sib_out, own_sib.at[0], UP_PARTS)
    down_args = (down, down_in, down_sib, down_out, down_sib_out, own_sib.at[1], DOWN_PARTS)
    for k, buf in enumerate((up, down)):
        remote(buf.at[z, c], buf.at[z, c], own_sib_out, own_sib.at[k], tp=sibling).start()

    @pl.when(home)
    def _():
        for k in range(TOKEN_PARTS):
            remote(tok.at[token_rows(k)], seen.at[token_rows(k)], tok_out, tok_in.at[k], grp=partner).start()

    begin(*up_args)
    acc[...] = jnp.zeros_like(acc)
    squares[...] = jnp.zeros_like(squares)

    def normalize(k):
        arrived(seen.at[token_rows(k)], tok_in.at[k])
        step = 32

        def body(i, _):
            view = pl.ds(pl.multiple_of(k * tok_rows + i * step, step), step)
            values = seen[view, :].astype(jnp.float32)
            mean = jnp.mean(values * values, axis=-1, keepdims=True)
            scaled = (values * lax.rsqrt(mean + epsilon) * gain[...]).astype(jnp.bfloat16)
            for q in range(n_quads):
                normed[q, view, :] = scaled[:, q * quad : (q + 1) * quad]
            return 0

        lax.fori_loop(0, tok_rows // step, body, 0)

    def lift(i, _):
        m = jnp.where(c == 0, pick(LIFTS[0], i), pick(LIFTS[1], i))
        q = lax.rem(z_quad - way * m + n_quads + 8, n_quads)
        from_sibling(q, up, up_sib)
        for h in range(2):
            weights = up[pl.ds(4 * q, 4), h].reshape(quad, mine)
            acc[h] += jnp.dot(normed[q], weights, preferred_element_type=jnp.float32)
        return 0

    def activate():
        for h in range(2):
            hidden[h] = jnp.square(jnp.maximum(acc[h], 0.0)).astype(jnp.bfloat16)

    def project(j, _):
        q = quad_of(j)

        @pl.when(lax.rem(j, 2) == 0)
        def _():
            from_sibling(q, down, down_sib)

        total = None
        for h in range(2):
            weights = down[pl.ds(4 * q, 4), h].reshape(quad, mine)
            term = lax.dot_general(
                hidden[h, chunk_rows(j), :], weights, (((1,), (1,)), ((), ())), preferred_element_type=jnp.float32
            )
            total = term if total is None else total + term
        part[j] = total.astype(jnp.bfloat16)

        @pl.when(jnp.logical_not(home))
        def _():
            remote(part.at[j], ypart.at[j], y_out, y_in.at[j], grp=partner).start()

        return 0

    def pair_sum(j):
        arrived(ypart.at[j], y_in.at[j])
        part[j] = (part[j].astype(jnp.float32) + ypart[j].astype(jnp.float32)).astype(jnp.bfloat16)
        for i in range(1, nx):
            view = pl.ds(pl.multiple_of(peer(i) * own, own), own)
            slot = nx - 1 - i
            remote(
                part.at[j, view], xpart.at[j, slot], x_out, x_in.at[j], tp=2 * peer(i) + c
            ).start()

    def row_sum(j):
        q = quad_of(j)
        total = part[j, pl.ds(pl.multiple_of(x * own, own), own), :].astype(jnp.float32)
        arrived(xpart.at[j], x_in.at[j])
        for i in range(nx - 1):
            total += xpart[j, i].astype(jnp.float32)
        branch[q, chunk_rows(j, x), :] = total.astype(jnp.bfloat16)
        view = branch.at[q, chunk_rows(j, x)]
        for i in (1, nx - 1):
            remote(view, view, all_out, all_in.at[j], tp=2 * peer(i) + c).start()
        remote(view, view, all_sib_out, branch_sib.at[j], tp=sibling).start()

    def pass_on(i, j):
        view = branch.at[quad_of(j), chunk_rows(j, peer(i))]
        remote(view, view, all_sib_out, branch_sib.at[j], tp=sibling).start()
        return view

    def hand_on(j):
        arrived(part.at[j, pl.ds(0, 2 * own)], all_in.at[j])
        view = pass_on(1, j)
        remote(view, view, all_out, all_in.at[n_chunks + j], tp=2 * peer(nx - 1) + c).start()
        pass_on(nx - 1, j)

    def write(j):
        view = (quad_of(j), chunk_rows(j))
        pltpu.make_async_copy(branch.at[view], out.at[view], out_sem).start()
        values = branch[view[0], view[1], :].astype(jnp.float32)
        values *= values
        lanes = squares.shape[1]
        squares[view[1], :] += sum(values[:, k : k + lanes] for k in range(0, quad, lanes))

    def hand_far(j):
        arrived(part.at[j, pl.ds(0, own)], all_in.at[n_chunks + j])
        pass_on(2, j)
        write(j)

    stages = ((1, pair_sum), (4, row_sum), (7, hand_on), (10, hand_far))

    def tick(i, _):
        for behind, stage in stages:

            @pl.when((i >= behind) & (i < n_chunks + behind))
            def _():
                stage(i - behind)

        return 0

    ready = jnp.where(c == 0, 1, 0)
    ticks_at = jnp.where(c == 0, TICKS[0], TICKS[1])

    def lifts_at(over):
        return jnp.where((c == 1) & (over > 0), n_quads, jnp.clip(2 * over + 4, 0, n_quads))

    norm_at = 8 + 3 * c

    def ring_pass(s, _):
        @pl.when(s <= last)
        def _():
            ring_step(s, *up_args)

        @pl.when(s == lag)
        def _():
            begin(*down_args)

        @pl.when(s > lag)
        def _():
            ring_step(s - lag, *down_args)

        @pl.when((s >= norm_at) & (s < norm_at + TOKEN_PARTS))
        def _():
            normalize(s - norm_at)

        over = s - last

        lo, hi = lifts_at(over), lifts_at(over + 1)

        @pl.when(near & (hi > lo))
        def _():
            lax.fori_loop(lo, hi, lift, 0)

        @pl.when(near & (over == ready))
        def _():
            activate()

        @pl.when(near & (over > ready))
        def _():
            lax.fori_loop(2 * (over - ready) - 2, 2 * (over - ready), project, 0)

        @pl.when(near & home & (over >= ticks_at))
        def _():
            lax.fori_loop(2 * (over - ticks_at) + 1, 2 * (over - ticks_at) + 3, tick, 0)

        return 0

    lax.fori_loop(1, last + lag + 1, ring_pass, 0)

    @pl.when(jnp.logical_not(near))
    def _():
        lax.fori_loop(0, n_quads, lift, 0)
        activate()

    made = jnp.where(near, 2 * (lag - ready), 0)
    ticked = jnp.where(near, 2 * (lag - ticks_at + 1) + 1, 0)

    def output_pass(i, _):
        @pl.when(made + i < n_chunks)
        def _():
            project(made + i, 0)

        @pl.when(home)
        def _():
            tick(ticked + i, 0)

        return 0

    lax.fori_loop(0, n_chunks + stages[-1][0], output_pass, 0)

    for side in range(2):

        @pl.when(c == side)
        def _():
            for sem in (up_out, down_out, up_sib_out, down_sib_out):
                arrived(up.at[pl.ds(0, reach[side])], sem)

    arrived(up.at[0], own_sib_out)

    @pl.when(home)
    def _():
        arrived(seen, tok_out)
        most = part.at[pl.ds(0, n_chunks * (nx - 1) // nx)]
        arrived(most, x_out)
        arrived(most, all_out)
        arrived(part, all_sib_out)

    @pl.when(jnp.logical_not(home))
    def _():
        arrived(part, y_out)

        def write_arrived(j, _):
            arrived(part.at[j], branch_sib.at[j])
            write(j)
            return 0

        lax.fori_loop(0, n_chunks, write_arrived, 0)

    total = jnp.sum(squares[...], axis=-1, keepdims=True)
    squares[...] = jnp.broadcast_to(lax.rsqrt(total / width + epsilon), squares.shape)
    written = pltpu.make_async_copy(squares, scale_out, scale_sem)
    written.start()
    arrived(part, out_sem)
    written.wait()


def finish(branch, scale, tok, post, out, branch_v, scale_v, tok_v, out_v, came, left):
    n_quads, rows, quad = branch.shape
    lanes = scale.shape[1]
    tall = rows // FINISH_PARTS

    def reads(k):
        view = pl.ds(k * tall, tall)
        return [
            pltpu.make_async_copy(branch.at[:, view], branch_v.at[:, view], came.at[3 * k]),
            pltpu.make_async_copy(scale.at[view], scale_v.at[view], came.at[3 * k + 1]),
            pltpu.make_async_copy(tok.at[view], tok_v.at[view], came.at[3 * k + 2]),
        ]

    for k in range(FINISH_PARTS):
        for copy in reads(k):
            copy.start()
    writes = []
    for k in range(FINISH_PARTS):
        view = slice(k * tall, (k + 1) * tall)
        for copy in reads(k):
            copy.wait()
        for q in range(n_quads):
            for i in range(0, quad, lanes):
                cols = slice(q * quad + i, q * quad + i + lanes)
                values = branch_v[q, view, i : i + lanes].astype(jnp.float32) * scale_v[view, :] * post[:, cols]
                out_v[view, cols] = (tok_v[view, cols].astype(jnp.float32) + values).astype(jnp.bfloat16)
        writes.append(pltpu.make_async_copy(out_v.at[view], out.at[view], left.at[k]))
        writes[-1].start()
    for copy in writes:
        copy.wait()


def solution(mesh):
    nz, nx = mesh.shape["fs"], mesh.shape["tp"] // 2

    def on_device(tokens, pre_gain, up_weight, up_scale, down_weight, down_scale, post_gain):
        rows, width = tokens.shape
        block, units = up_weight.shape
        mine = units // 2
        quad = 4 * block
        n_quads = width // quad
        n_chunks = 2 * n_quads
        tall = rows // 2
        own = tall // nx
        longest = max(reaches(nz))
        bf16, f32 = jnp.bfloat16, jnp.float32
        dma = pltpu.SemaphoreType.DMA
        anywhere = pl.BlockSpec(memory_space=pl.ANY)
        branch, scale = pl.pallas_call(
            functools.partial(kernel, nz, nx),
            out_shape=(
                jax.ShapeDtypeStruct((n_quads, rows, quad), bf16),
                jax.ShapeDtypeStruct((rows, 128), f32),
            ),
            in_specs=[anywhere] * 6,
            out_specs=(anywhere, anywhere),
            scratch_shapes=[
                pltpu.VMEM((1, width), f32),
                pltpu.VMEM((block, units), f32),
                pltpu.VMEM((1, units), f32),
                pltpu.VMEM((block, units), f32),
                pltpu.VMEM((1, block), f32),
                pltpu.VMEM((rows, 128), f32),
                pltpu.VMEM((nz, 2, block, mine), bf16),
                pltpu.VMEM((nz, 2, block, mine), bf16),
                pltpu.VMEM((rows, width), bf16),
                pltpu.VMEM((n_quads, rows, quad), bf16),
                pltpu.VMEM((2, rows, mine), f32),
                pltpu.VMEM((2, rows, mine), bf16),
                pltpu.VMEM((n_chunks, tall, quad), bf16),
                pltpu.VMEM((n_chunks, tall, quad), bf16),
                pltpu.VMEM((n_chunks, nx - 1, own, quad), bf16),
                pltpu.VMEM((n_quads, rows, quad), bf16),
                dma((longest * 2 * UP_PARTS,)),
                dma((longest * 2 * DOWN_PARTS,)),
                dma((n_quads,)),
                dma((n_quads,)),
                dma((2,)),
                dma((TOKEN_PARTS,)),
                dma((n_chunks,)),
                dma((n_chunks,)),
                dma((2 * n_chunks,)),
                dma((n_chunks,)),
                dma,
                dma,
                dma,
                dma,
                dma,
                dma,
                dma,
                dma,
                dma,
                dma,
                dma,
                dma((5,)),
                dma,
            ],
            compiler_params=pltpu.CompilerParams(
                collective_id=0, has_side_effects=True, vmem_limit_bytes=60 * 1024 * 1024
            ),
        )(
            tokens,
            pre_gain.reshape(1, width),
            up_weight,
            up_scale.reshape(1, units),
            down_weight.T,
            down_scale.reshape(1, block),
        )
        return pl.pallas_call(
            finish,
            out_shape=jax.ShapeDtypeStruct((rows, width), bf16),
            in_specs=[anywhere] * 3 + [pl.BlockSpec(memory_space=pltpu.VMEM)],
            out_specs=anywhere,
            scratch_shapes=[
                pltpu.VMEM((n_quads, rows, quad), bf16),
                pltpu.VMEM((rows, 128), f32),
                pltpu.VMEM((rows, width), bf16),
                pltpu.VMEM((rows, width), bf16),
                dma((3 * FINISH_PARTS,)),
                dma((FINISH_PARTS,)),
            ],
            compiler_params=pltpu.CompilerParams(vmem_limit_bytes=60 * 1024 * 1024),
        )(branch, scale, tokens, post_gain.reshape(1, width))

    placed = (P(("grp", "fs"), None), P(), P("fs", "tp"), P("tp"), P("tp", "fs"), P("fs"), P())
    return jax.shard_map(
        on_device, mesh=mesh, in_specs=placed, out_specs=P(("grp", "fs"), None), check_vma=False
    )
```

```python
import functools

import jax
import jax.numpy as jnp
from jax import lax
from jax.experimental import pallas as pl
from jax.experimental.pallas import tpu as pltpu
from jax.sharding import PartitionSpec as P

epsilon = 1e-06
MESH = pl.DeviceIdType.MESH

LAG = (10, 6)
UP_PARTS, DOWN_PARTS = 4, 2
TICKS = (4, 2)
EARLY = (5, 6)
TOKEN_PARTS = 4
FINISH_PARTS = 4
LIFTS = ((1, 8, 2, 7, 6, 5, 3, 4), (1, 8, 2, 7, 3, 6, 5, 4))
ORDER = (1, 2, 0, 3, 7, 6, 4, 5)


def remote(src, dst, send_sem, recv_sem, **where):
    return pltpu.make_async_remote_copy(
        src_ref=src, dst_ref=dst, send_sem=send_sem, recv_sem=recv_sem, device_id=where, device_id_type=MESH
    )


def arrived(ref, sem):
    pltpu.make_async_copy(ref, ref, sem).wait()


def reaches(nz):
    return nz * 13 // 32, nz - 1 - nz * 13 // 32


def kernel(
    nz, nx, tok, gain_in, up_w_in, up_s_in, down_w_in, down_s_in, out, scale_out,
    gain, up_w, up_s, down_w, down_s, squares, up, down, seen, normed, acc, hidden, part, ypart, xpart, branch,
    up_in, down_in, up_sib, down_sib, own_sib, tok_in, y_in, x_in, all_in, branch_sib,
    up_out, down_out, up_sib_out, down_sib_out, own_sib_out, tok_out, y_out, x_out, all_out, all_sib_out, out_sem, fetched, scale_sem,
):
    rows, width = tok.shape
    block, units = up_w_in.shape
    mine = units // 2
    quad = 4 * block
    n_quads = width // quad
    n_chunks = 2 * n_quads
    tall = rows // 2
    own = tall // nx
    tok_rows = rows // TOKEN_PARTS
    reach = reaches(nz)

    g = lax.axis_index("grp")
    z = lax.axis_index("fs")
    t = lax.axis_index("tp")
    y = lax.rem(g, 2)
    c = lax.rem(t, 2)
    x = t // 2
    partner = g + 1 - 2 * y
    sibling = t + 1 - 2 * c
    way = 1 - 2 * c
    following = lax.rem(z + way + nz, nz)
    previous = lax.rem(z - way + nz, nz)
    home = c == y
    z_quad = z // 4
    last = jnp.where(c == 0, reach[0], reach[1])
    lag = jnp.where(c == 0, LAG[0], LAG[1])
    near = (z < nz * 3 // 4) | (c == 1)

    def peer(i):
        return lax.rem(x + i, nx)

    fetches = [
        pltpu.make_async_copy(src, dst, fetched.at[k])
        for k, (src, dst) in enumerate(
            ((up_w_in, up_w), (up_s_in, up_s), (down_w_in, down_w), (down_s_in, down_s), (gain_in, gain))
        )
    ]
    for fetch in fetches:
        fetch.start()
    barrier = pltpu.get_barrier_semaphore()
    neighbours = [{"fs": previous}, {"tp": sibling}, {"grp": partner}]
    neighbours += [{"tp": 2 * peer(i) + c} for i in range(1, nx)]
    for where in neighbours:
        pl.semaphore_signal(barrier, inc=1, device_id=where, device_id_type=MESH)

    def token_rows(k):
        return pl.ds(pl.multiple_of(k * tok_rows, tok_rows), tok_rows)

    @pl.when(home)
    def _():
        for k in range(TOKEN_PARTS):
            pltpu.make_async_copy(tok.at[token_rows(k)], seen.at[token_rows(k)], tok_in.at[k]).start()

    for fetch in fetches:
        fetch.wait()
    half = pl.ds(pl.multiple_of(y * mine, mine), mine)
    up[z, c] = (up_w[:, half] * up_s[:, half]).astype(jnp.bfloat16)
    line = lax.broadcasted_iota(jnp.int32, (block, block), 0) == lax.broadcasted_iota(jnp.int32, (block, block), 1)
    column = jnp.sum(jnp.where(line, jnp.broadcast_to(down_s[...], (block, block)), 0.0), axis=1, keepdims=True)
    down[z, c] = (down_w[:, half] * column).astype(jnp.bfloat16)
    pl.semaphore_wait(barrier, len(neighbours))

    def pick(values, i):
        return sum(jnp.where(i == k, v, 0) for k, v in enumerate(values))

    def quad_of(j):
        return lax.rem(z_quad + pick(ORDER, j // 2), n_quads)

    def chunk_rows(j, of=None):
        first = lax.rem(j, 2) * tall
        if of is None:
            return pl.ds(pl.multiple_of(first, tall), tall)
        return pl.ds(pl.multiple_of(first + of * own, own), own)

    def send_half(s, b, h, buf, in_sem, out_sem, parts):
        piece = block // parts
        for k in range(parts):
            view = buf.at[b, h, pl.ds(k * piece, piece)]

            def slot(step):
                return in_sem.at[(2 * (step - 1) + h) * parts + k]

            if s is None:
                remote(view, view, out_sem, slot(1), fs=following).start()
                continue
            arrived(view, slot(s))

            @pl.when(s < last)
            def _():
                remote(view, view, out_sem, slot(s + 1), fs=following).start()

    def begin(buf, in_sem, sib_sem, out_sem, sib_out, own_sem, parts):
        send_half(None, z, c, buf, in_sem, out_sem, parts)
        arrived(buf.at[z, 1 - c], own_sem)
        send_half(None, z, 1 - c, buf, in_sem, out_sem, parts)

    def ring_step(s, buf, in_sem, sib_sem, out_sem, sib_out, own_sem, parts):
        b = lax.rem(z - way * s + nz, nz)
        for h in (c, 1 - c):
            send_half(s, b, h, buf, in_sem, out_sem, parts)
        remote(buf.at[b], buf.at[b], sib_out, sib_sem.at[b // 4], tp=sibling).start()

    def from_sibling(q, buf, sib_sem):
        count = 0
        for i in range(4):
            ahead = lax.rem(4 * q + i - z + nz, nz)
            theirs = (ahead > 0) & jnp.where(c == 0, ahead <= reach[1], ahead > reach[1])
            count += jnp.where(theirs, 1, 0)
        for n in range(1, 5):

            @pl.when(count == n)
            def _():
                arrived(buf.at[pl.ds(0, n)], sib_sem.at[q])

    up_args = (up, up_in, up_sib, up_out, up_sib_out, own_sib.at[0], UP_PARTS)
    down_args = (down, down_in, down_sib, down_out, down_sib_out, own_sib.at[1], DOWN_PARTS)
    for k, buf in enumerate((up, down)):
        remote(buf.at[z, c], buf.at[z, c], own_sib_out, own_sib.at[k], tp=sibling).start()

    @pl.when(home)
    def _():
        for k in range(TOKEN_PARTS):
            remote(tok.at[token_rows(k)], seen.at[token_rows(k)], tok_out, tok_in.at[k], grp=partner).start()

    begin(*up_args)
    acc[...] = jnp.zeros_like(acc)
    squares[...] = jnp.zeros_like(squares)

    def normalize(k):
        arrived(seen.at[token_rows(k)], tok_in.at[k])
        step = 32

        def body(i, _):
            view = pl.ds(pl.multiple_of(k * tok_rows + i * step, step), step)
            values = seen[view, :].astype(jnp.float32)
            mean = jnp.mean(values * values, axis=-1, keepdims=True)
            scaled = (values * lax.rsqrt(mean + epsilon) * gain[...]).astype(jnp.bfloat16)
            for q in range(n_quads):
                normed[q, view, :] = scaled[:, q * quad : (q + 1) * quad]
            return 0

        lax.fori_loop(0, tok_rows // step, body, 0)

    def lift(i, _):
        m = jnp.where(c == 0, pick(LIFTS[0], i), pick(LIFTS[1], i))
        q = lax.rem(z_quad - way * m + n_quads + 8, n_quads)
        from_sibling(q, up, up_sib)
        for h in range(2):
            weights = up[pl.ds(4 * q, 4), h].reshape(quad, mine)
            acc[h] += jnp.dot(normed[q], weights, preferred_element_type=jnp.float32)
        return 0

    def activate():
        for h in range(2):
            hidden[h] = jnp.square(jnp.maximum(acc[h], 0.0)).astype(jnp.bfloat16)

    def project(j, _):
        q = quad_of(j)

        @pl.when(lax.rem(j, 2) == 0)
        def _():
            from_sibling(q, down, down_sib)

        total = None
        for h in range(2):
            weights = down[pl.ds(4 * q, 4), h].reshape(quad, mine)
            term = lax.dot_general(
                hidden[h, chunk_rows(j), :], weights, (((1,), (1,)), ((), ())), preferred_element_type=jnp.float32
            )
            total = term if total is None else total + term
        part[j] = total.astype(jnp.bfloat16)

        @pl.when(jnp.logical_not(home))
        def _():
            remote(part.at[j], ypart.at[j], y_out, y_in.at[j], grp=partner).start()

        return 0

    def pair_sum(j):
        arrived(ypart.at[j], y_in.at[j])
        part[j] = (part[j].astype(jnp.float32) + ypart[j].astype(jnp.float32)).astype(jnp.bfloat16)
        for i in range(1, nx):
            view = pl.ds(pl.multiple_of(peer(i) * own, own), own)
            slot = nx - 1 - i
            remote(
                part.at[j, view], xpart.at[j, slot], x_out, x_in.at[j], tp=2 * peer(i) + c
            ).start()

    def row_sum(j):
        q = quad_of(j)
        total = part[j, pl.ds(pl.multiple_of(x * own, own), own), :].astype(jnp.float32)
        arrived(xpart.at[j], x_in.at[j])
        for i in range(nx - 1):
            total += xpart[j, i].astype(jnp.float32)
        branch[q, chunk_rows(j, x), :] = total.astype(jnp.bfloat16)
        view = branch.at[q, chunk_rows(j, x)]
        for i in (1, nx - 1):
            remote(view, view, all_out, all_in.at[j], tp=2 * peer(i) + c).start()
        remote(view, view, all_sib_out, branch_sib.at[j], tp=sibling).start()

    def pass_on(i, j):
        view = branch.at[quad_of(j), chunk_rows(j, peer(i))]
        remote(view, view, all_sib_out, branch_sib.at[j], tp=sibling).start()
        return view

    def hand_on(j):
        arrived(part.at[j, pl.ds(0, 2 * own)], all_in.at[j])
        view = pass_on(1, j)
        remote(view, view, all_out, all_in.at[n_chunks + j], tp=2 * peer(nx - 1) + c).start()
        pass_on(nx - 1, j)

    def write(j):
        view = (quad_of(j), chunk_rows(j))
        pltpu.make_async_copy(branch.at[view], out.at[view], out_sem).start()
        values = branch[view[0], view[1], :].astype(jnp.float32)
        values *= values
        lanes = squares.shape[1]
        squares[view[1], :] += sum(values[:, k : k + lanes] for k in range(0, quad, lanes))

    def hand_far(j):
        arrived(part.at[j, pl.ds(0, own)], all_in.at[n_chunks + j])
        pass_on(2, j)
        write(j)

    stages = ((1, pair_sum), (4, row_sum), (7, hand_on), (10, hand_far))

    def tick(i, _):
        for behind, stage in stages:

            @pl.when((i >= behind) & (i < n_chunks + behind))
            def _():
                stage(i - behind)

        return 0

    ready = jnp.where(c == 0, 1, 0)
    ticks_at = jnp.where(c == 0, TICKS[0], TICKS[1])
    early = jnp.where(c == 0, EARLY[0], EARLY[1])

    def lifts_at(over):
        return jnp.where((c == 1) & (over > 0), n_quads, jnp.clip(2 * over + 4, 0, n_quads))

    norm_at = 8 + 3 * c

    def ring_pass(s, _):
        @pl.when(s <= last)
        def _():
            ring_step(s, *up_args)

        @pl.when(s == lag)
        def _():
            begin(*down_args)

        @pl.when(s > lag)
        def _():
            ring_step(s - lag, *down_args)

        @pl.when((s >= norm_at) & (s < norm_at + TOKEN_PARTS))
        def _():
            normalize(s - norm_at)

        over = s - last

        lo, hi = lifts_at(over), lifts_at(over + 1)

        @pl.when(near & (hi > lo))
        def _():
            lax.fori_loop(lo, hi, lift, 0)

        @pl.when(near & (over == ready))
        def _():
            activate()

        @pl.when(near & (over > ready) & (over <= ready + early))
        def _():
            lax.fori_loop(2 * (over - ready) - 2, 2 * (over - ready), project, 0)

        @pl.when(near & home & (over >= ticks_at) & (over < ticks_at + early))
        def _():
            lax.fori_loop(2 * (over - ticks_at) + 1, 2 * (over - ticks_at) + 3, tick, 0)

        return 0

    lax.fori_loop(1, last + lag + 1, ring_pass, 0)

    @pl.when(jnp.logical_not(near))
    def _():
        lax.fori_loop(0, n_quads, lift, 0)
        activate()

    made = jnp.where(near, 2 * early, 0)
    ticked = jnp.where(near, 2 * jnp.minimum(early, lag - ticks_at + 1) + 1, 0)

    def output_pass(i, _):
        @pl.when(made + i < n_chunks)
        def _():
            project(made + i, 0)

        @pl.when(home)
        def _():
            tick(ticked + i, 0)

        return 0

    lax.fori_loop(0, n_chunks + stages[-1][0], output_pass, 0)

    for side in range(2):

        @pl.when(c == side)
        def _():
            for sem in (up_out, down_out, up_sib_out, down_sib_out):
                arrived(up.at[pl.ds(0, reach[side])], sem)

    arrived(up.at[0], own_sib_out)

    @pl.when(home)
    def _():
        arrived(seen, tok_out)
        most = part.at[pl.ds(0, n_chunks * (nx - 1) // nx)]
        arrived(most, x_out)
        arrived(most, all_out)
        arrived(part, all_sib_out)

    @pl.when(jnp.logical_not(home))
    def _():
        arrived(part, y_out)

        def write_arrived(j, _):
            arrived(part.at[j], branch_sib.at[j])
            write(j)
            return 0

        lax.fori_loop(0, n_chunks, write_arrived, 0)

    total = jnp.sum(squares[...], axis=-1, keepdims=True)
    squares[...] = jnp.broadcast_to(lax.rsqrt(total / width + epsilon), squares.shape)
    written = pltpu.make_async_copy(squares, scale_out, scale_sem)
    written.start()
    arrived(part, out_sem)
    written.wait()


def finish(branch, scale, tok, post, out, branch_v, scale_v, tok_v, out_v, came, left):
    n_quads, rows, quad = branch.shape
    lanes = scale.shape[1]
    tall = rows // FINISH_PARTS

    def reads(k):
        view = pl.ds(k * tall, tall)
        return [
            pltpu.make_async_copy(branch.at[:, view], branch_v.at[:, view], came.at[3 * k]),
            pltpu.make_async_copy(scale.at[view], scale_v.at[view], came.at[3 * k + 1]),
            pltpu.make_async_copy(tok.at[view], tok_v.at[view], came.at[3 * k + 2]),
        ]

    for k in range(FINISH_PARTS):
        for copy in reads(k):
            copy.start()
    writes = []
    for k in range(FINISH_PARTS):
        view = slice(k * tall, (k + 1) * tall)
        for copy in reads(k):
            copy.wait()
        for q in range(n_quads):
            for i in range(0, quad, lanes):
                cols = slice(q * quad + i, q * quad + i + lanes)
                values = branch_v[q, view, i : i + lanes].astype(jnp.float32) * scale_v[view, :] * post[:, cols]
                out_v[view, cols] = (tok_v[view, cols].astype(jnp.float32) + values).astype(jnp.bfloat16)
        writes.append(pltpu.make_async_copy(out_v.at[view], out.at[view], left.at[k]))
        writes[-1].start()
    for copy in writes:
        copy.wait()


def solution(mesh):
    nz, nx = mesh.shape["fs"], mesh.shape["tp"] // 2

    def on_device(tokens, pre_gain, up_weight, up_scale, down_weight, down_scale, post_gain):
        rows, width = tokens.shape
        block, units = up_weight.shape
        mine = units // 2
        quad = 4 * block
        n_quads = width // quad
        n_chunks = 2 * n_quads
        tall = rows // 2
        own = tall // nx
        longest = max(reaches(nz))
        bf16, f32 = jnp.bfloat16, jnp.float32
        dma = pltpu.SemaphoreType.DMA
        anywhere = pl.BlockSpec(memory_space=pl.ANY)
        branch, scale = pl.pallas_call(
            functools.partial(kernel, nz, nx),
            out_shape=(
                jax.ShapeDtypeStruct((n_quads, rows, quad), bf16),
                jax.ShapeDtypeStruct((rows, 128), f32),
            ),
            in_specs=[anywhere] * 6,
            out_specs=(anywhere, anywhere),
            scratch_shapes=[
                pltpu.VMEM((1, width), f32),
                pltpu.VMEM((block, units), f32),
                pltpu.VMEM((1, units), f32),
                pltpu.VMEM((block, units), f32),
                pltpu.VMEM((1, block), f32),
                pltpu.VMEM((rows, 128), f32),
                pltpu.VMEM((nz, 2, block, mine), bf16),
                pltpu.VMEM((nz, 2, block, mine), bf16),
                pltpu.VMEM((rows, width), bf16),
                pltpu.VMEM((n_quads, rows, quad), bf16),
                pltpu.VMEM((2, rows, mine), f32),
                pltpu.VMEM((2, rows, mine), bf16),
                pltpu.VMEM((n_chunks, tall, quad), bf16),
                pltpu.VMEM((n_chunks, tall, quad), bf16),
                pltpu.VMEM((n_chunks, nx - 1, own, quad), bf16),
                pltpu.VMEM((n_quads, rows, quad), bf16),
                dma((longest * 2 * UP_PARTS,)),
                dma((longest * 2 * DOWN_PARTS,)),
                dma((n_quads,)),
                dma((n_quads,)),
                dma((2,)),
                dma((TOKEN_PARTS,)),
                dma((n_chunks,)),
                dma((n_chunks,)),
                dma((2 * n_chunks,)),
                dma((n_chunks,)),
                dma,
                dma,
                dma,
                dma,
                dma,
                dma,
                dma,
                dma,
                dma,
                dma,
                dma,
                dma((5,)),
                dma,
            ],
            compiler_params=pltpu.CompilerParams(
                collective_id=0, has_side_effects=True, vmem_limit_bytes=60 * 1024 * 1024
            ),
        )(
            tokens,
            pre_gain.reshape(1, width),
            up_weight,
            up_scale.reshape(1, units),
            down_weight.T,
            down_scale.reshape(1, block),
        )
        return pl.pallas_call(
            finish,
            out_shape=jax.ShapeDtypeStruct((rows, width), bf16),
            in_specs=[anywhere] * 3 + [pl.BlockSpec(memory_space=pltpu.VMEM)],
            out_specs=anywhere,
            scratch_shapes=[
                pltpu.VMEM((n_quads, rows, quad), bf16),
                pltpu.VMEM((rows, 128), f32),
                pltpu.VMEM((rows, width), bf16),
                pltpu.VMEM((rows, width), bf16),
                dma((3 * FINISH_PARTS,)),
                dma((FINISH_PARTS,)),
            ],
            compiler_params=pltpu.CompilerParams(vmem_limit_bytes=60 * 1024 * 1024),
        )(branch, scale, tokens, post_gain.reshape(1, width))

    placed = (P(("grp", "fs"), None), P(), P("fs", "tp"), P("tp"), P("tp", "fs"), P("fs"), P())
    return jax.shard_map(
        on_device, mesh=mesh, in_specs=placed, out_specs=P(("grp", "fs"), None), check_vma=False
    )
```

```python
import functools

import jax
import jax.numpy as jnp
from jax import lax
from jax.experimental import pallas as pl
from jax.experimental.pallas import tpu as pltpu
from jax.sharding import PartitionSpec as P

epsilon = 1e-06
MESH = pl.DeviceIdType.MESH

LAG = (8, 6)
UP_PARTS, DOWN_PARTS = 4, 2
TICKS = (3, 1)
EARLY = (6, 6)
TOKEN_PARTS = 4
FINISH_PARTS = 4
LIFTS = ((1, 8, 2, 7, 6, 5, 3, 4), (1, 8, 2, 7, 3, 6, 5, 4))
ORDER = (1, 2, 0, 3, 7, 6, 4, 5)


def remote(src, dst, send_sem, recv_sem, **where):
    return pltpu.make_async_remote_copy(
        src_ref=src, dst_ref=dst, send_sem=send_sem, recv_sem=recv_sem, device_id=where, device_id_type=MESH
    )


def arrived(ref, sem):
    pltpu.make_async_copy(ref, ref, sem).wait()


def reaches(nz):
    return nz * 13 // 32, nz - 1 - nz * 13 // 32


def kernel(
    nz, nx, tok, gain_in, up_w_in, up_s_in, down_w_in, down_s_in, out, scale_out,
    gain, up_w, up_s, down_w, down_s, squares, up, down, seen, normed, acc, hidden, part, ypart, xpart, branch,
    up_in, down_in, up_sib, down_sib, own_sib, tok_in, y_in, x_in, all_in, branch_sib,
    up_out, down_out, up_sib_out, down_sib_out, own_sib_out, tok_out, y_out, x_out, all_out, all_sib_out, out_sem, fetched, scale_sem,
):
    rows, width = tok.shape
    block, units = up_w_in.shape
    mine = units // 2
    quad = 4 * block
    n_quads = width // quad
    n_chunks = 2 * n_quads
    tall = rows // 2
    own = tall // nx
    tok_rows = rows // TOKEN_PARTS
    reach = reaches(nz)

    g = lax.axis_index("grp")
    z = lax.axis_index("fs")
    t = lax.axis_index("tp")
    y = lax.rem(g, 2)
    c = lax.rem(t, 2)
    x = t // 2
    partner = g + 1 - 2 * y
    sibling = t + 1 - 2 * c
    way = 1 - 2 * c
    following = lax.rem(z + way + nz, nz)
    previous = lax.rem(z - way + nz, nz)
    home = c == y
    z_quad = z // 4
    last = jnp.where(c == 0, reach[0], reach[1])
    lag = jnp.where(c == 0, LAG[0], LAG[1])
    near = (z < nz * 3 // 4) | (c == 1)

    def peer(i):
        return lax.rem(x + i, nx)

    fetches = [
        pltpu.make_async_copy(src, dst, fetched.at[k])
        for k, (src, dst) in enumerate(
            ((up_w_in, up_w), (up_s_in, up_s), (down_w_in, down_w), (down_s_in, down_s), (gain_in, gain))
        )
    ]
    for fetch in fetches:
        fetch.start()
    barrier = pltpu.get_barrier_semaphore()
    neighbours = [{"fs": previous}, {"tp": sibling}, {"grp": partner}]
    neighbours += [{"tp": 2 * peer(i) + c} for i in range(1, nx)]
    for where in neighbours:
        pl.semaphore_signal(barrier, inc=1, device_id=where, device_id_type=MESH)

    def token_rows(k):
        return pl.ds(pl.multiple_of(k * tok_rows, tok_rows), tok_rows)

    @pl.when(home)
    def _():
        for k in range(TOKEN_PARTS):
            pltpu.make_async_copy(tok.at[token_rows(k)], seen.at[token_rows(k)], tok_in.at[k]).start()

    for fetch in fetches:
        fetch.wait()
    half = pl.ds(pl.multiple_of(y * mine, mine), mine)
    up[z, c] = (up_w[:, half] * up_s[:, half]).astype(jnp.bfloat16)
    line = lax.broadcasted_iota(jnp.int32, (block, block), 0) == lax.broadcasted_iota(jnp.int32, (block, block), 1)
    column = jnp.sum(jnp.where(line, jnp.broadcast_to(down_s[...], (block, block)), 0.0), axis=1, keepdims=True)
    down[z, c] = (down_w[:, half] * column).astype(jnp.bfloat16)
    pl.semaphore_wait(barrier, len(neighbours))

    def pick(values, i):
        return sum(jnp.where(i == k, v, 0) for k, v in enumerate(values))

    def quad_of(j):
        return lax.rem(z_quad + pick(ORDER, j // 2), n_quads)

    def chunk_rows(j, of=None):
        first = lax.rem(j, 2) * tall
        if of is None:
            return pl.ds(pl.multiple_of(first, tall), tall)
        return pl.ds(pl.multiple_of(first + of * own, own), own)

    def send_half(s, b, h, buf, in_sem, out_sem, parts):
        piece = block // parts
        for k in range(parts):
            view = buf.at[b, h, pl.ds(k * piece, piece)]

            def slot(step):
                return in_sem.at[(2 * (step - 1) + h) * parts + k]

            if s is None:
                remote(view, view, out_sem, slot(1), fs=following).start()
                continue
            arrived(view, slot(s))

            @pl.when(s < last)
            def _():
                remote(view, view, out_sem, slot(s + 1), fs=following).start()

    def begin(buf, in_sem, sib_sem, out_sem, sib_out, own_sem, parts):
        send_half(None, z, c, buf, in_sem, out_sem, parts)
        arrived(buf.at[z, 1 - c], own_sem)
        send_half(None, z, 1 - c, buf, in_sem, out_sem, parts)

    def ring_step(s, buf, in_sem, sib_sem, out_sem, sib_out, own_sem, parts):
        b = lax.rem(z - way * s + nz, nz)
        for h in (c, 1 - c):
            send_half(s, b, h, buf, in_sem, out_sem, parts)
        remote(buf.at[b], buf.at[b], sib_out, sib_sem.at[b // 4], tp=sibling).start()

    def from_sibling(q, buf, sib_sem):
        count = 0
        for i in range(4):
            ahead = lax.rem(4 * q + i - z + nz, nz)
            theirs = (ahead > 0) & jnp.where(c == 0, ahead <= reach[1], ahead > reach[1])
            count += jnp.where(theirs, 1, 0)
        for n in range(1, 5):

            @pl.when(count == n)
            def _():
                arrived(buf.at[pl.ds(0, n)], sib_sem.at[q])

    up_args = (up, up_in, up_sib, up_out, up_sib_out, own_sib.at[0], UP_PARTS)
    down_args = (down, down_in, down_sib, down_out, down_sib_out, own_sib.at[1], DOWN_PARTS)
    for k, buf in enumerate((up, down)):
        remote(buf.at[z, c], buf.at[z, c], own_sib_out, own_sib.at[k], tp=sibling).start()

    @pl.when(home)
    def _():
        for k in range(TOKEN_PARTS):
            remote(tok.at[token_rows(k)], seen.at[token_rows(k)], tok_out, tok_in.at[k], grp=partner).start()

    begin(*up_args)
    acc[...] = jnp.zeros_like(acc)
    squares[...] = jnp.zeros_like(squares)

    def normalize(k):
        arrived(seen.at[token_rows(k)], tok_in.at[k])
        step = 32

        def body(i, _):
            view = pl.ds(pl.multiple_of(k * tok_rows + i * step, step), step)
            values = seen[view, :].astype(jnp.float32)
            mean = jnp.mean(values * values, axis=-1, keepdims=True)
            scaled = (values * lax.rsqrt(mean + epsilon) * gain[...]).astype(jnp.bfloat16)
            for q in range(n_quads):
                normed[q, view, :] = scaled[:, q * quad : (q + 1) * quad]
            return 0

        lax.fori_loop(0, tok_rows // step, body, 0)

    def lift(i, _):
        m = jnp.where(c == 0, pick(LIFTS[0], i), pick(LIFTS[1], i))
        q = lax.rem(z_quad - way * m + n_quads + 8, n_quads)
        from_sibling(q, up, up_sib)
        for h in range(2):
            weights = up[pl.ds(4 * q, 4), h].reshape(quad, mine)
            acc[h] += jnp.dot(normed[q], weights, preferred_element_type=jnp.float32)
        return 0

    def activate():
        for h in range(2):
            hidden[h] = jnp.square(jnp.maximum(acc[h], 0.0)).astype(jnp.bfloat16)

    def project(j, _):
        q = quad_of(j)

        @pl.when(lax.rem(j, 2) == 0)
        def _():
            from_sibling(q, down, down_sib)

        total = None
        for h in range(2):
            weights = down[pl.ds(4 * q, 4), h].reshape(quad, mine)
            term = lax.dot_general(
                hidden[h, chunk_rows(j), :], weights, (((1,), (1,)), ((), ())), preferred_element_type=jnp.float32
            )
            total = term if total is None else total + term
        part[j] = total.astype(jnp.bfloat16)

        @pl.when(jnp.logical_not(home))
        def _():
            remote(part.at[j], ypart.at[j], y_out, y_in.at[j], grp=partner).start()

        return 0

    def pair_sum(j):
        arrived(ypart.at[j], y_in.at[j])
        part[j] = (part[j].astype(jnp.float32) + ypart[j].astype(jnp.float32)).astype(jnp.bfloat16)
        for i in range(1, nx):
            view = pl.ds(pl.multiple_of(peer(i) * own, own), own)
            slot = nx - 1 - i
            remote(
                part.at[j, view], xpart.at[j, slot], x_out, x_in.at[j], tp=2 * peer(i) + c
            ).start()

    def row_sum(j):
        q = quad_of(j)
        total = part[j, pl.ds(pl.multiple_of(x * own, own), own), :].astype(jnp.float32)
        arrived(xpart.at[j], x_in.at[j])
        for i in range(nx - 1):
            total += xpart[j, i].astype(jnp.float32)
        branch[q, chunk_rows(j, x), :] = total.astype(jnp.bfloat16)
        view = branch.at[q, chunk_rows(j, x)]
        for i in (1, nx - 1):
            remote(view, view, all_out, all_in.at[j], tp=2 * peer(i) + c).start()
        remote(view, view, all_sib_out, branch_sib.at[j], tp=sibling).start()

    def pass_on(i, j):
        view = branch.at[quad_of(j), chunk_rows(j, peer(i))]
        remote(view, view, all_sib_out, branch_sib.at[j], tp=sibling).start()
        return view

    def hand_on(j):
        arrived(part.at[j, pl.ds(0, 2 * own)], all_in.at[j])
        view = pass_on(1, j)
        remote(view, view, all_out, all_in.at[n_chunks + j], tp=2 * peer(nx - 1) + c).start()
        pass_on(nx - 1, j)

    def write(j):
        view = (quad_of(j), chunk_rows(j))
        pltpu.make_async_copy(branch.at[view], out.at[view], out_sem).start()
        values = branch[view[0], view[1], :].astype(jnp.float32)
        values *= values
        lanes = squares.shape[1]
        squares[view[1], :] += sum(values[:, k : k + lanes] for k in range(0, quad, lanes))

    def hand_far(j):
        arrived(part.at[j, pl.ds(0, own)], all_in.at[n_chunks + j])
        pass_on(2, j)
        write(j)

    stages = ((1, pair_sum), (4, row_sum), (7, hand_on), (10, hand_far))

    def tick(i, _):
        for behind, stage in stages:

            @pl.when((i >= behind) & (i < n_chunks + behind))
            def _():
                stage(i - behind)

        return 0

    ready = jnp.where(c == 0, 1, 0)
    ticks_at = jnp.where(c == 0, TICKS[0], TICKS[1])
    early = jnp.where(c == 0, EARLY[0], EARLY[1])

    def lifts_at(over):
        return jnp.where((c == 1) & (over > 0), n_quads, jnp.clip(2 * over + 4, 0, n_quads))

    norm_at = 8 + 3 * c

    def ring_pass(s, _):
        @pl.when(s <= last)
        def _():
            ring_step(s, *up_args)

        @pl.when(s == lag)
        def _():
            begin(*down_args)

        @pl.when(s > lag)
        def _():
            ring_step(s - lag, *down_args)

        @pl.when((s >= norm_at) & (s < norm_at + TOKEN_PARTS))
        def _():
            normalize(s - norm_at)

        over = s - last

        lo, hi = lifts_at(over), lifts_at(over + 1)

        @pl.when(near & (hi > lo))
        def _():
            lax.fori_loop(lo, hi, lift, 0)

        @pl.when(near & (over == ready))
        def _():
            activate()

        @pl.when(near & (over >= ready) & (over < ready + early))
        def _():
            lax.fori_loop(2 * (over - ready), 2 * (over - ready) + 2, project, 0)

        @pl.when(near & home & (over >= ticks_at) & (over < ticks_at + early))
        def _():
            lax.fori_loop(2 * (over - ticks_at) + 1, 2 * (over - ticks_at) + 3, tick, 0)

        return 0

    lax.fori_loop(1, last + lag + 1, ring_pass, 0)

    @pl.when(jnp.logical_not(near))
    def _():
        lax.fori_loop(0, n_quads, lift, 0)
        activate()

    made = jnp.where(near, 2 * early, 0)
    ticked = jnp.where(near, 2 * jnp.minimum(early, lag - ticks_at + 1) + 1, 0)

    def output_pass(i, _):
        @pl.when(made + i < n_chunks)
        def _():
            project(made + i, 0)

        @pl.when(home)
        def _():
            tick(ticked + i, 0)

        return 0

    lax.fori_loop(0, n_chunks + stages[-1][0], output_pass, 0)

    for side in range(2):

        @pl.when(c == side)
        def _():
            for sem in (up_out, down_out, up_sib_out, down_sib_out):
                arrived(up.at[pl.ds(0, reach[side])], sem)

    arrived(up.at[0], own_sib_out)

    @pl.when(home)
    def _():
        arrived(seen, tok_out)
        most = part.at[pl.ds(0, n_chunks * (nx - 1) // nx)]
        arrived(most, x_out)
        arrived(most, all_out)
        arrived(part, all_sib_out)

    @pl.when(jnp.logical_not(home))
    def _():
        arrived(part, y_out)

        def write_arrived(j, _):
            arrived(part.at[j], branch_sib.at[j])
            write(j)
            return 0

        lax.fori_loop(0, n_chunks, write_arrived, 0)

    total = jnp.sum(squares[...], axis=-1, keepdims=True)
    squares[...] = jnp.broadcast_to(lax.rsqrt(total / width + epsilon), squares.shape)
    written = pltpu.make_async_copy(squares, scale_out, scale_sem)
    written.start()
    arrived(part, out_sem)
    written.wait()


def finish(branch, scale, tok, post, out, branch_v, scale_v, tok_v, out_v, came, left):
    n_quads, rows, quad = branch.shape
    lanes = scale.shape[1]
    tall = rows // FINISH_PARTS

    def reads(k):
        view = pl.ds(k * tall, tall)
        return [
            pltpu.make_async_copy(branch.at[:, view], branch_v.at[:, view], came.at[3 * k]),
            pltpu.make_async_copy(scale.at[view], scale_v.at[view], came.at[3 * k + 1]),
            pltpu.make_async_copy(tok.at[view], tok_v.at[view], came.at[3 * k + 2]),
        ]

    for k in range(FINISH_PARTS):
        for copy in reads(k):
            copy.start()
    writes = []
    for k in range(FINISH_PARTS):
        view = slice(k * tall, (k + 1) * tall)
        for copy in reads(k):
            copy.wait()
        for q in range(n_quads):
            for i in range(0, quad, lanes):
                cols = slice(q * quad + i, q * quad + i + lanes)
                values = branch_v[q, view, i : i + lanes].astype(jnp.float32) * scale_v[view, :] * post[:, cols]
                out_v[view, cols] = (tok_v[view, cols].astype(jnp.float32) + values).astype(jnp.bfloat16)
        writes.append(pltpu.make_async_copy(out_v.at[view], out.at[view], left.at[k]))
        writes[-1].start()
    for copy in writes:
        copy.wait()


def solution(mesh):
    nz, nx = mesh.shape["fs"], mesh.shape["tp"] // 2

    def on_device(tokens, pre_gain, up_weight, up_scale, down_weight, down_scale, post_gain):
        rows, width = tokens.shape
        block, units = up_weight.shape
        mine = units // 2
        quad = 4 * block
        n_quads = width // quad
        n_chunks = 2 * n_quads
        tall = rows // 2
        own = tall // nx
        longest = max(reaches(nz))
        bf16, f32 = jnp.bfloat16, jnp.float32
        dma = pltpu.SemaphoreType.DMA
        anywhere = pl.BlockSpec(memory_space=pl.ANY)
        branch, scale = pl.pallas_call(
            functools.partial(kernel, nz, nx),
            out_shape=(
                jax.ShapeDtypeStruct((n_quads, rows, quad), bf16),
                jax.ShapeDtypeStruct((rows, 128), f32),
            ),
            in_specs=[anywhere] * 6,
            out_specs=(anywhere, anywhere),
            scratch_shapes=[
                pltpu.VMEM((1, width), f32),
                pltpu.VMEM((block, units), f32),
                pltpu.VMEM((1, units), f32),
                pltpu.VMEM((block, units), f32),
                pltpu.VMEM((1, block), f32),
                pltpu.VMEM((rows, 128), f32),
                pltpu.VMEM((nz, 2, block, mine), bf16),
                pltpu.VMEM((nz, 2, block, mine), bf16),
                pltpu.VMEM((rows, width), bf16),
                pltpu.VMEM((n_quads, rows, quad), bf16),
                pltpu.VMEM((2, rows, mine), f32),
                pltpu.VMEM((2, rows, mine), bf16),
                pltpu.VMEM((n_chunks, tall, quad), bf16),
                pltpu.VMEM((n_chunks, tall, quad), bf16),
                pltpu.VMEM((n_chunks, nx - 1, own, quad), bf16),
                pltpu.VMEM((n_quads, rows, quad), bf16),
                dma((longest * 2 * UP_PARTS,)),
                dma((longest * 2 * DOWN_PARTS,)),
                dma((n_quads,)),
                dma((n_quads,)),
                dma((2,)),
                dma((TOKEN_PARTS,)),
                dma((n_chunks,)),
                dma((n_chunks,)),
                dma((2 * n_chunks,)),
                dma((n_chunks,)),
                dma,
                dma,
                dma,
                dma,
                dma,
                dma,
                dma,
                dma,
                dma,
                dma,
                dma,
                dma((5,)),
                dma,
            ],
            compiler_params=pltpu.CompilerParams(
                collective_id=0, has_side_effects=True, vmem_limit_bytes=60 * 1024 * 1024
            ),
        )(
            tokens,
            pre_gain.reshape(1, width),
            up_weight,
            up_scale.reshape(1, units),
            down_weight.T,
            down_scale.reshape(1, block),
        )
        return pl.pallas_call(
            finish,
            out_shape=jax.ShapeDtypeStruct((rows, width), bf16),
            in_specs=[anywhere] * 3 + [pl.BlockSpec(memory_space=pltpu.VMEM)],
            out_specs=anywhere,
            scratch_shapes=[
                pltpu.VMEM((n_quads, rows, quad), bf16),
                pltpu.VMEM((rows, 128), f32),
                pltpu.VMEM((rows, width), bf16),
                pltpu.VMEM((rows, width), bf16),
                dma((3 * FINISH_PARTS,)),
                dma((FINISH_PARTS,)),
            ],
            compiler_params=pltpu.CompilerParams(vmem_limit_bytes=60 * 1024 * 1024),
        )(branch, scale, tokens, post_gain.reshape(1, width))

    placed = (P(("grp", "fs"), None), P(), P("fs", "tp"), P("tp"), P("tp", "fs"), P("fs"), P())
    return jax.shard_map(
        on_device, mesh=mesh, in_specs=placed, out_specs=P(("grp", "fs"), None), check_vma=False
    )
```

```python
import functools

import jax
import jax.numpy as jnp
from jax import lax
from jax.experimental import pallas as pl
from jax.experimental.pallas import tpu as pltpu
from jax.sharding import PartitionSpec as P

epsilon = 1e-06
MESH = pl.DeviceIdType.MESH

LAG = (8, 6)
UP_PARTS, DOWN_PARTS = 2, 2
TICKS = (3, 1)
EARLY = (6, 6)
TOKEN_PARTS = 4
FINISH_PARTS = 4
LIFTS = ((1, 8, 2, 7, 6, 5, 3, 4), (1, 8, 2, 7, 3, 6, 5, 4))
ORDER = (1, 2, 0, 3, 7, 6, 4, 5)


def remote(src, dst, send_sem, recv_sem, **where):
    return pltpu.make_async_remote_copy(
        src_ref=src, dst_ref=dst, send_sem=send_sem, recv_sem=recv_sem, device_id=where, device_id_type=MESH
    )


def arrived(ref, sem):
    pltpu.make_async_copy(ref, ref, sem).wait()


def reaches(nz):
    return nz * 13 // 32, nz - 1 - nz * 13 // 32


def kernel(
    nz, nx, tok, gain_in, up_w_in, up_s_in, down_w_in, down_s_in, out, scale_out,
    gain, up_w, up_s, down_w, down_s, squares, up, down, seen, normed, acc, hidden, part, ypart, xpart, branch,
    up_in, down_in, up_sib, down_sib, own_sib, tok_in, y_in, x_in, all_in, branch_sib,
    up_out, down_out, up_sib_out, down_sib_out, own_sib_out, tok_out, y_out, x_out, all_out, all_sib_out, out_sem, fetched, scale_sem,
):
    rows, width = tok.shape
    block, units = up_w_in.shape
    mine = units // 2
    quad = 4 * block
    n_quads = width // quad
    n_chunks = 2 * n_quads
    tall = rows // 2
    own = tall // nx
    tok_rows = rows // TOKEN_PARTS
    reach = reaches(nz)

    g = lax.axis_index("grp")
    z = lax.axis_index("fs")
    t = lax.axis_index("tp")
    y = lax.rem(g, 2)
    c = lax.rem(t, 2)
    x = t // 2
    partner = g + 1 - 2 * y
    sibling = t + 1 - 2 * c
    way = 1 - 2 * c
    following = lax.rem(z + way + nz, nz)
    previous = lax.rem(z - way + nz, nz)
    home = c == y
    z_quad = z // 4
    last = jnp.where(c == 0, reach[0], reach[1])
    lag = jnp.where(c == 0, LAG[0], LAG[1])
    near = (z < nz * 3 // 4) | (c == 1)

    def peer(i):
        return lax.rem(x + i, nx)

    fetches = [
        pltpu.make_async_copy(src, dst, fetched.at[k])
        for k, (src, dst) in enumerate(
            ((up_w_in, up_w), (up_s_in, up_s), (down_w_in, down_w), (down_s_in, down_s), (gain_in, gain))
        )
    ]
    for fetch in fetches:
        fetch.start()
    barrier = pltpu.get_barrier_semaphore()
    neighbours = [{"fs": previous}, {"tp": sibling}, {"grp": partner}]
    neighbours += [{"tp": 2 * peer(i) + c} for i in range(1, nx)]
    for where in neighbours:
        pl.semaphore_signal(barrier, inc=1, device_id=where, device_id_type=MESH)

    def token_rows(k):
        return pl.ds(pl.multiple_of(k * tok_rows, tok_rows), tok_rows)

    @pl.when(home)
    def _():
        for k in range(TOKEN_PARTS):
            pltpu.make_async_copy(tok.at[token_rows(k)], seen.at[token_rows(k)], tok_in.at[k]).start()

    for fetch in fetches:
        fetch.wait()
    half = pl.ds(pl.multiple_of(y * mine, mine), mine)
    up[z, c] = (up_w[:, half] * up_s[:, half]).astype(jnp.bfloat16)
    line = lax.broadcasted_iota(jnp.int32, (block, block), 0) == lax.broadcasted_iota(jnp.int32, (block, block), 1)
    column = jnp.sum(jnp.where(line, jnp.broadcast_to(down_s[...], (block, block)), 0.0), axis=1, keepdims=True)
    down[z, c] = (down_w[:, half] * column).astype(jnp.bfloat16)
    pl.semaphore_wait(barrier, len(neighbours))

    def pick(values, i):
        return sum(jnp.where(i == k, v, 0) for k, v in enumerate(values))

    def quad_of(j):
        return lax.rem(z_quad + pick(ORDER, j // 2), n_quads)

    def chunk_rows(j, of=None):
        first = lax.rem(j, 2) * tall
        if of is None:
            return pl.ds(pl.multiple_of(first, tall), tall)
        return pl.ds(pl.multiple_of(first + of * own, own), own)

    def send_half(s, b, h, buf, in_sem, out_sem, parts):
        piece = block // parts
        for k in range(parts):
            view = buf.at[b, h, pl.ds(k * piece, piece)]

            def slot(step):
                return in_sem.at[(2 * (step - 1) + h) * parts + k]

            if s is None:
                remote(view, view, out_sem, slot(1), fs=following).start()
                continue
            arrived(view, slot(s))

            @pl.when(s < last)
            def _():
                remote(view, view, out_sem, slot(s + 1), fs=following).start()

    def begin(buf, in_sem, sib_sem, out_sem, sib_out, own_sem, parts):
        send_half(None, z, c, buf, in_sem, out_sem, parts)
        arrived(buf.at[z, 1 - c], own_sem)
        send_half(None, z, 1 - c, buf, in_sem, out_sem, parts)

    def ring_step(s, buf, in_sem, sib_sem, out_sem, sib_out, own_sem, parts):
        b = lax.rem(z - way * s + nz, nz)
        for h in (c, 1 - c):
            send_half(s, b, h, buf, in_sem, out_sem, parts)
        remote(buf.at[b], buf.at[b], sib_out, sib_sem.at[b // 4], tp=sibling).start()

    def from_sibling(q, buf, sib_sem):
        count = 0
        for i in range(4):
            ahead = lax.rem(4 * q + i - z + nz, nz)
            theirs = (ahead > 0) & jnp.where(c == 0, ahead <= reach[1], ahead > reach[1])
            count += jnp.where(theirs, 1, 0)
        for n in range(1, 5):

            @pl.when(count == n)
            def _():
                arrived(buf.at[pl.ds(0, n)], sib_sem.at[q])

    up_args = (up, up_in, up_sib, up_out, up_sib_out, own_sib.at[0], UP_PARTS)
    down_args = (down, down_in, down_sib, down_out, down_sib_out, own_sib.at[1], DOWN_PARTS)
    for k, buf in enumerate((up, down)):
        remote(buf.at[z, c], buf.at[z, c], own_sib_out, own_sib.at[k], tp=sibling).start()

    @pl.when(home)
    def _():
        for k in range(TOKEN_PARTS):
            remote(tok.at[token_rows(k)], seen.at[token_rows(k)], tok_out, tok_in.at[k], grp=partner).start()

    begin(*up_args)
    acc[...] = jnp.zeros_like(acc)
    squares[...] = jnp.zeros_like(squares)

    def normalize(k):
        arrived(seen.at[token_rows(k)], tok_in.at[k])
        step = 32

        def body(i, _):
            view = pl.ds(pl.multiple_of(k * tok_rows + i * step, step), step)
            values = seen[view, :].astype(jnp.float32)
            mean = jnp.mean(values * values, axis=-1, keepdims=True)
            scaled = (values * lax.rsqrt(mean + epsilon) * gain[...]).astype(jnp.bfloat16)
            for q in range(n_quads):
                normed[q, view, :] = scaled[:, q * quad : (q + 1) * quad]
            return 0

        lax.fori_loop(0, tok_rows // step, body, 0)

    def lift(i, _):
        m = jnp.where(c == 0, pick(LIFTS[0], i), pick(LIFTS[1], i))
        q = lax.rem(z_quad - way * m + n_quads + 8, n_quads)
        from_sibling(q, up, up_sib)
        for h in range(2):
            weights = up[pl.ds(4 * q, 4), h].reshape(quad, mine)
            acc[h] += jnp.dot(normed[q], weights, preferred_element_type=jnp.float32)
        return 0

    def activate():
        for h in range(2):
            hidden[h] = jnp.square(jnp.maximum(acc[h], 0.0)).astype(jnp.bfloat16)

    def project(j, _):
        q = quad_of(j)

        @pl.when(lax.rem(j, 2) == 0)
        def _():
            from_sibling(q, down, down_sib)

        total = None
        for h in range(2):
            weights = down[pl.ds(4 * q, 4), h].reshape(quad, mine)
            term = lax.dot_general(
                hidden[h, chunk_rows(j), :], weights, (((1,), (1,)), ((), ())), preferred_element_type=jnp.float32
            )
            total = term if total is None else total + term
        part[j] = total.astype(jnp.bfloat16)

        @pl.when(jnp.logical_not(home))
        def _():
            remote(part.at[j], ypart.at[j], y_out, y_in.at[j], grp=partner).start()

        return 0

    def pair_sum(j):
        arrived(ypart.at[j], y_in.at[j])
        part[j] = (part[j].astype(jnp.float32) + ypart[j].astype(jnp.float32)).astype(jnp.bfloat16)
        for i in range(1, nx):
            view = pl.ds(pl.multiple_of(peer(i) * own, own), own)
            slot = nx - 1 - i
            remote(
                part.at[j, view], xpart.at[j, slot], x_out, x_in.at[j], tp=2 * peer(i) + c
            ).start()

    def row_sum(j):
        q = quad_of(j)
        total = part[j, pl.ds(pl.multiple_of(x * own, own), own), :].astype(jnp.float32)
        arrived(xpart.at[j], x_in.at[j])
        for i in range(nx - 1):
            total += xpart[j, i].astype(jnp.float32)
        branch[q, chunk_rows(j, x), :] = total.astype(jnp.bfloat16)
        view = branch.at[q, chunk_rows(j, x)]
        for i in (1, nx - 1):
            remote(view, view, all_out, all_in.at[j], tp=2 * peer(i) + c).start()
        remote(view, view, all_sib_out, branch_sib.at[j], tp=sibling).start()

    def pass_on(i, j):
        view = branch.at[quad_of(j), chunk_rows(j, peer(i))]
        remote(view, view, all_sib_out, branch_sib.at[j], tp=sibling).start()
        return view

    def hand_on(j):
        arrived(part.at[j, pl.ds(0, 2 * own)], all_in.at[j])
        view = pass_on(1, j)
        remote(view, view, all_out, all_in.at[n_chunks + j], tp=2 * peer(nx - 1) + c).start()
        pass_on(nx - 1, j)

    def write(j):
        view = (quad_of(j), chunk_rows(j))
        pltpu.make_async_copy(branch.at[view], out.at[view], out_sem).start()
        values = branch[view[0], view[1], :].astype(jnp.float32)
        values *= values
        lanes = squares.shape[1]
        squares[view[1], :] += sum(values[:, k : k + lanes] for k in range(0, quad, lanes))

    def hand_far(j):
        arrived(part.at[j, pl.ds(0, own)], all_in.at[n_chunks + j])
        pass_on(2, j)
        write(j)

    stages = ((1, pair_sum), (4, row_sum), (7, hand_on), (10, hand_far))

    def tick(i, _):
        for behind, stage in stages:

            @pl.when((i >= behind) & (i < n_chunks + behind))
            def _():
                stage(i - behind)

        return 0

    ready = jnp.where(c == 0, 1, 0)
    ticks_at = jnp.where(c == 0, TICKS[0], TICKS[1])
    early = jnp.where(c == 0, EARLY[0], EARLY[1])

    def lifts_at(over):
        return jnp.where((c == 1) & (over > 0), n_quads, jnp.clip(2 * over + 4, 0, n_quads))

    norm_at = 8 + 3 * c

    def ring_pass(s, _):
        @pl.when(s <= last)
        def _():
            ring_step(s, *up_args)

        @pl.when(s == lag)
        def _():
            begin(*down_args)

        @pl.when(s > lag)
        def _():
            ring_step(s - lag, *down_args)

        @pl.when((s >= norm_at) & (s < norm_at + TOKEN_PARTS))
        def _():
            normalize(s - norm_at)

        over = s - last

        lo, hi = lifts_at(over), lifts_at(over + 1)

        @pl.when(near & (hi > lo))
        def _():
            lax.fori_loop(lo, hi, lift, 0)

        @pl.when(near & (over == ready))
        def _():
            activate()

        @pl.when(near & (over >= ready) & (over < ready + early))
        def _():
            lax.fori_loop(2 * (over - ready), 2 * (over - ready) + 2, project, 0)

        @pl.when(near & home & (over >= ticks_at) & (over < ticks_at + early))
        def _():
            lax.fori_loop(2 * (over - ticks_at) + 1, 2 * (over - ticks_at) + 3, tick, 0)

        return 0

    lax.fori_loop(1, last + lag + 1, ring_pass, 0)

    @pl.when(jnp.logical_not(near))
    def _():
        lax.fori_loop(0, n_quads, lift, 0)
        activate()

    made = jnp.where(near, 2 * early, 0)
    ticked = jnp.where(near, 2 * jnp.minimum(early, lag - ticks_at + 1) + 1, 0)

    def output_pass(i, _):
        @pl.when(made + i < n_chunks)
        def _():
            project(made + i, 0)

        @pl.when(home)
        def _():
            tick(ticked + i, 0)

        return 0

    lax.fori_loop(0, n_chunks + stages[-1][0], output_pass, 0)

    for side in range(2):

        @pl.when(c == side)
        def _():
            for sem in (up_out, down_out, up_sib_out, down_sib_out):
                arrived(up.at[pl.ds(0, reach[side])], sem)

    arrived(up.at[0], own_sib_out)

    @pl.when(home)
    def _():
        arrived(seen, tok_out)
        most = part.at[pl.ds(0, n_chunks * (nx - 1) // nx)]
        arrived(most, x_out)
        arrived(most, all_out)
        arrived(part, all_sib_out)

    @pl.when(jnp.logical_not(home))
    def _():
        arrived(part, y_out)

        def write_arrived(j, _):
            arrived(part.at[j], branch_sib.at[j])
            write(j)
            return 0

        lax.fori_loop(0, n_chunks, write_arrived, 0)

    total = jnp.sum(squares[...], axis=-1, keepdims=True)
    squares[...] = jnp.broadcast_to(lax.rsqrt(total / width + epsilon), squares.shape)
    written = pltpu.make_async_copy(squares, scale_out, scale_sem)
    written.start()
    arrived(part, out_sem)
    written.wait()


def finish(branch, scale, tok, post, out, branch_v, scale_v, tok_v, out_v, came, left):
    n_quads, rows, quad = branch.shape
    lanes = scale.shape[1]
    tall = rows // FINISH_PARTS

    def reads(k):
        view = pl.ds(k * tall, tall)
        return [
            pltpu.make_async_copy(branch.at[:, view], branch_v.at[:, view], came.at[3 * k]),
            pltpu.make_async_copy(scale.at[view], scale_v.at[view], came.at[3 * k + 1]),
            pltpu.make_async_copy(tok.at[view], tok_v.at[view], came.at[3 * k + 2]),
        ]

    for k in range(FINISH_PARTS):
        for copy in reads(k):
            copy.start()
    writes = []
    for k in range(FINISH_PARTS):
        view = slice(k * tall, (k + 1) * tall)
        for copy in reads(k):
            copy.wait()
        for q in range(n_quads):
            for i in range(0, quad, lanes):
                cols = slice(q * quad + i, q * quad + i + lanes)
                values = branch_v[q, view, i : i + lanes].astype(jnp.float32) * scale_v[view, :] * post[:, cols]
                out_v[view, cols] = (tok_v[view, cols].astype(jnp.float32) + values).astype(jnp.bfloat16)
        writes.append(pltpu.make_async_copy(out_v.at[view], out.at[view], left.at[k]))
        writes[-1].start()
    for copy in writes:
        copy.wait()


def solution(mesh):
    nz, nx = mesh.shape["fs"], mesh.shape["tp"] // 2

    def on_device(tokens, pre_gain, up_weight, up_scale, down_weight, down_scale, post_gain):
        rows, width = tokens.shape
        block, units = up_weight.shape
        mine = units // 2
        quad = 4 * block
        n_quads = width // quad
        n_chunks = 2 * n_quads
        tall = rows // 2
        own = tall // nx
        longest = max(reaches(nz))
        bf16, f32 = jnp.bfloat16, jnp.float32
        dma = pltpu.SemaphoreType.DMA
        anywhere = pl.BlockSpec(memory_space=pl.ANY)
        branch, scale = pl.pallas_call(
            functools.partial(kernel, nz, nx),
            out_shape=(
                jax.ShapeDtypeStruct((n_quads, rows, quad), bf16),
                jax.ShapeDtypeStruct((rows, 128), f32),
            ),
            in_specs=[anywhere] * 6,
            out_specs=(anywhere, anywhere),
            scratch_shapes=[
                pltpu.VMEM((1, width), f32),
                pltpu.VMEM((block, units), f32),
                pltpu.VMEM((1, units), f32),
                pltpu.VMEM((block, units), f32),
                pltpu.VMEM((1, block), f32),
                pltpu.VMEM((rows, 128), f32),
                pltpu.VMEM((nz, 2, block, mine), bf16),
                pltpu.VMEM((nz, 2, block, mine), bf16),
                pltpu.VMEM((rows, width), bf16),
                pltpu.VMEM((n_quads, rows, quad), bf16),
                pltpu.VMEM((2, rows, mine), f32),
                pltpu.VMEM((2, rows, mine), bf16),
                pltpu.VMEM((n_chunks, tall, quad), bf16),
                pltpu.VMEM((n_chunks, tall, quad), bf16),
                pltpu.VMEM((n_chunks, nx - 1, own, quad), bf16),
                pltpu.VMEM((n_quads, rows, quad), bf16),
                dma((longest * 2 * UP_PARTS,)),
                dma((longest * 2 * DOWN_PARTS,)),
                dma((n_quads,)),
                dma((n_quads,)),
                dma((2,)),
                dma((TOKEN_PARTS,)),
                dma((n_chunks,)),
                dma((n_chunks,)),
                dma((2 * n_chunks,)),
                dma((n_chunks,)),
                dma,
                dma,
                dma,
                dma,
                dma,
                dma,
                dma,
                dma,
                dma,
                dma,
                dma,
                dma((5,)),
                dma,
            ],
            compiler_params=pltpu.CompilerParams(
                collective_id=0, has_side_effects=True, vmem_limit_bytes=60 * 1024 * 1024
            ),
        )(
            tokens,
            pre_gain.reshape(1, width),
            up_weight,
            up_scale.reshape(1, units),
            down_weight.T,
            down_scale.reshape(1, block),
        )
        return pl.pallas_call(
            finish,
            out_shape=jax.ShapeDtypeStruct((rows, width), bf16),
            in_specs=[anywhere] * 3 + [pl.BlockSpec(memory_space=pltpu.VMEM)],
            out_specs=anywhere,
            scratch_shapes=[
                pltpu.VMEM((n_quads, rows, quad), bf16),
                pltpu.VMEM((rows, 128), f32),
                pltpu.VMEM((rows, width), bf16),
                pltpu.VMEM((rows, width), bf16),
                dma((3 * FINISH_PARTS,)),
                dma((FINISH_PARTS,)),
            ],
            compiler_params=pltpu.CompilerParams(vmem_limit_bytes=60 * 1024 * 1024),
        )(branch, scale, tokens, post_gain.reshape(1, width))

    placed = (P(("grp", "fs"), None), P(), P("fs", "tp"), P("tp"), P("tp", "fs"), P("fs"), P())
    return jax.shard_map(
        on_device, mesh=mesh, in_specs=placed, out_specs=P(("grp", "fs"), None), check_vma=False
    )
```
